256 devices in a mesh: sp: 32 (over z, y), tp: 8 (over x, core).
Axes of the slice: x: 4, y: 4, z: 8, core: 2. Of those that a mesh axis runs over, the one named last changes fastest.
Arguments:
- hidden_states: bfloat16 [8192, 4096], P('sp', 'tp'), may hold values from -6 to 6
- norm_gain: float32 [4096], replicated, may hold values from 0.1 to 1.9
- query_weight: bfloat16 [4096, 2048], P('sp', 'tp'), may hold values from -0.09375 to 0.09375
- key_weight: bfloat16 [4096, 2048], P('sp', 'tp'), may hold values from -0.09375 to 0.09375
- value_weight: bfloat16 [4096, 2048], P('sp', 'tp'), may hold values from -0.09375 to 0.09375
- output_gate_weight: bfloat16 [4096, 2048], P('sp', 'tp'), may hold values from -0.09375 to 0.09375
- unit_input_weight: bfloat16 [4096, 2048], P('sp', 'tp'), may hold values from -0.09375 to 0.09375
- unit_gate_weight: bfloat16 [4096, 2048], P('sp', 'tp'), may hold values from -0.09375 to 0.09375
- decay_forward: float32 [16], P('tp'), may hold values from 0 to 16
- decay_backward: float32 [16], P('tp'), may hold values from 0 to 16
- group_gain: float32 [2048], P('tp'), may hold values from 0.1 to 1.9
- group_bias: float32 [2048], P('tp'), may hold values from -3 to 3
- depth_kernel: float32 [31, 2048], P(None, 'tp'), may hold values from -7 to 7
- depth_bias: float32 [2048], P('tp'), may hold values from -3 to 3
- channel_gain: float32 [2048], P('tp'), may hold values from 0.1 to 1.9
- channel_bias: float32 [2048], P('tp'), may hold values from -3 to 3
- retention_out_weight: bfloat16 [2048, 4096], P('tp', 'sp'), may hold values from -0.09375 to 0.09375
- convolution_out_weight: bfloat16 [2048, 4096], P('tp', 'sp'), may hold values from -0.09375 to 0.09375
Outputs:
- mixed_out: bfloat16 [8192, 4096], P(('sp', 'tp'))
The draws below stay inside these ranges and needn't reach their ends.
All inputs are finite; a program needn't handle non-finite values.
Results may differ from the reference program's by a relative error of at most 0.018.
Values may be sent and summed in bfloat16 or wider, within the bound.
A program may use at most 128 MiB of HBM per device.

```python
import jax
import jax.numpy as jnp
from jax import lax

D = 4096
HEADS = 16
HEAD_DIM = 128
RET_WIDTH = 2048
CONV_WIDTH = 2048
KERNEL = 31
BLOCK = 128
TOKENS = 8192
N_TP = 8


def decay_logits(key, salt):
    key_pick, key_slow, key_fast = jax.random.split(jax.random.fold_in(key, salt), 3)
    keeps_state = jax.random.uniform(key_pick, (HEADS,), jnp.float32) < 0.5
    slow_rate = jnp.exp(jax.random.uniform(key_slow, (HEADS,), jnp.float32, jnp.log(0.2), jnp.log(2.0))) / TOKENS
    fast_rate = jnp.exp(jax.random.uniform(key_fast, (HEADS,), jnp.float32, jnp.log(1.0 / 100.0), jnp.log(1.0 / 30.0)))
    decay_rate = jnp.where(keeps_state, slow_rate, fast_rate)
    return -decay_rate - jnp.log(-jnp.expm1(-decay_rate))


def draw_decay_forward(key, part):
    return decay_logits(key, 11)


def draw_decay_backward(key, part):
    return decay_logits(key, 23)


def draw_depth_kernel(key, part):
    key_tap, key_spread = jax.random.split(jax.random.fold_in(key, 5))
    channel = jnp.arange(CONV_WIDTH, dtype=jnp.float32)
    rising = jnp.exp(jnp.log(3.0) * channel / CONV_WIDTH)
    spread = jnp.exp(jax.random.uniform(key_spread, (CONV_WIDTH,), jnp.float32, 0.0, jnp.log(4.0)))
    tap_values = jnp.clip(jax.random.normal(key_tap, (KERNEL, CONV_WIDTH), jnp.float32), -3.0, 3.0)
    return tap_values * (rising * spread)[None, :] / jnp.sqrt(jnp.float32(KERNEL))


def levels(own_key, shape, cuts, least, top_value):
    gain = 1.0
    for dim, blocks in cuts:
        heights = jax.random.uniform(jax.random.fold_in(jax.random.fold_in(own_key, 6), dim), (blocks,), jnp.float32, least / len(cuts), top_value / len(cuts))
        gain = gain * jnp.repeat(jnp.exp(heights), shape[dim] // blocks).reshape((-1,) + (1,) * (len(shape) - 1 - dim))
    return gain


def bell_draw(stream_key, extent, scale, most, shards=(), kind=jnp.bfloat16):
    entries = jax.random.normal(stream_key, extent, jnp.float32) * scale
    if len(shards) > 0:
        entries = levels(stream_key, extent, shards, -0.22, 0.18) * entries
    return jnp.clip(entries, min=-most, max=most).astype(kind)


def setup_inputs(seed: int = 0) -> dict:
    key_list = jax.random.split(jax.random.key(seed), 19)
    hidden_states = bell_draw(key_list[0], (TOKENS, D), 1.0, 6.0, ((0, 32), (1, 8)))
    norm_gain = jnp.clip(1.0 + 0.18 * jax.random.normal(key_list[1], (D,), jnp.float32), 0.1, 1.9)
    query_weight = bell_draw(key_list[2], (D, RET_WIDTH), D ** -0.5, 0.09375, ((0, 32), (1, 8)))
    key_weight = bell_draw(key_list[3], (D, RET_WIDTH), D ** -0.5, 0.09375, ((0, 32), (1, 8)))
    value_weight = bell_draw(key_list[4], (D, RET_WIDTH), D ** -0.5, 0.09375, ((0, 32), (1, 8)))
    output_gate_weight = bell_draw(key_list[5], (D, RET_WIDTH), D ** -0.5, 0.09375, ((0, 32), (1, 8)))
    unit_input_weight = bell_draw(key_list[6], (D, CONV_WIDTH), D ** -0.5, 0.09375, ((0, 32), (1, 8)))
    unit_gate_weight = bell_draw(key_list[7], (D, CONV_WIDTH), D ** -0.5, 0.09375, ((0, 32), (1, 8)))
    decay_forward = draw_decay_forward(jax.random.fold_in(key_list[18], 71), 0)
    decay_backward = draw_decay_backward(jax.random.fold_in(key_list[18], 71), 0)
    group_gain = jnp.clip(1.0 + 0.18 * jax.random.normal(key_list[10], (RET_WIDTH,), jnp.float32), 0.1, 1.9)
    group_bias = bell_draw(key_list[11], (RET_WIDTH,), 0.5, 3.0, ((0, 8),), jnp.float32)
    depth_kernel = draw_depth_kernel(jax.random.fold_in(key_list[18], 71), 0)
    depth_bias = bell_draw(key_list[13], (CONV_WIDTH,), 0.5, 3.0, ((0, 8),), jnp.float32)
    channel_gain = jnp.clip(1.0 + 0.18 * jax.random.normal(key_list[14], (CONV_WIDTH,), jnp.float32), 0.1, 1.9)
    channel_bias = bell_draw(key_list[15], (CONV_WIDTH,), 0.5, 3.0, ((0, 8),), jnp.float32)
    retention_out_weight = bell_draw(key_list[16], (RET_WIDTH, D), (RET_WIDTH + CONV_WIDTH) ** -0.5, 0.09375, ((0, 8), (1, 32)))
    convolution_out_weight = bell_draw(key_list[17], (CONV_WIDTH, D), (RET_WIDTH + CONV_WIDTH) ** -0.5, 0.09375, ((0, 8), (1, 32)))
    return dict(hidden_states=hidden_states, norm_gain=norm_gain, query_weight=query_weight, key_weight=key_weight, value_weight=value_weight, output_gate_weight=output_gate_weight, unit_input_weight=unit_input_weight, unit_gate_weight=unit_gate_weight, decay_forward=decay_forward, decay_backward=decay_backward, group_gain=group_gain, group_bias=group_bias, depth_kernel=depth_kernel, depth_bias=depth_bias, channel_gain=channel_gain, channel_bias=channel_bias, retention_out_weight=retention_out_weight, convolution_out_weight=convolution_out_weight)


EPS = 1e-06
THETA = 10000.0

def rotate(rows, positions):
    half_dim = rows.shape[-1] // 2
    inverse = THETA ** (-jnp.arange(half_dim, dtype=jnp.float32) / half_dim)
    angles = positions.astype(jnp.float32)[:, None] * inverse[None, :]
    cosine = jnp.cos(angles)[:, None, :]
    sine = jnp.sin(angles)[:, None, :]
    widened = rows.astype(jnp.float32)
    first_half = widened[..., :half_dim]
    second_half = widened[..., half_dim:]
    turned = jnp.concatenate([first_half * cosine - second_half * sine, second_half * cosine + first_half * sine], axis=-1)
    return turned.astype(jnp.bfloat16)

def to_blocks(rows):
    return rows.reshape(rows.shape[0] // BLOCK, BLOCK, rows.shape[1], rows.shape[2]).transpose(2, 0, 1, 3)

def from_blocks(blocks):
    return blocks.transpose(1, 2, 0, 3).reshape(blocks.shape[1] * blocks.shape[2], blocks.shape[0], blocks.shape[3])

def blockwise(queries, key_rows, values, log_decay, include_diag):
    block_len = queries.shape[2]
    position = jnp.arange(block_len, dtype=jnp.float32)
    distance = position[:, None] - position[None, :]
    allowed = distance >= 0 if include_diag else distance > 0
    inside = jnp.where(allowed[None], jnp.exp(log_decay[:, None, None] * jnp.maximum(distance, 0.0)[None]), 0.0)
    query_wide = queries.astype(jnp.float32)
    key_wide = key_rows.astype(jnp.float32)
    value_wide = values.astype(jnp.float32)
    scores = jnp.einsum('hnqd,hnkd->hnqk', query_wide, key_wide, precision=lax.Precision.HIGHEST) * inside[:, None]
    inner_part = jnp.einsum('hnqk,hnkd->hnqd', scores, value_wide, precision=lax.Precision.HIGHEST)
    toward_end = jnp.exp(log_decay[:, None] * (block_len - 1.0 - position)[None])
    block_states = jnp.einsum('hnkd,hnke->hnde', key_wide * toward_end[:, None, :, None], value_wide, precision=lax.Precision.HIGHEST)
    block_decay = jnp.exp(log_decay * block_len)[:, None, None]

    def advance(state_now, block_state):
        return (block_decay * state_now + block_state, state_now)
    initial = jnp.zeros((block_states.shape[0], block_states.shape[2], block_states.shape[3]), jnp.float32)
    final_state, earlier = lax.scan(advance, initial, jnp.moveaxis(block_states, 1, 0))
    earlier = jnp.moveaxis(earlier, 0, 1)
    from_start = jnp.exp(log_decay[:, None] * (position + 1.0)[None])
    cross_part = jnp.einsum('hnqd,hnde->hnqe', query_wide * from_start[:, None, :, None], earlier, precision=lax.Precision.HIGHEST)
    return (inner_part + cross_part, final_state)

def group_norm(retained, group_gain, group_bias, gate_rows):
    row_mean = lax.optimization_barrier(jnp.mean(retained, axis=-1, keepdims=True))
    centered = retained - row_mean
    variance = lax.optimization_barrier(jnp.mean(centered * centered, axis=-1, keepdims=True))
    scaled = (centered * lax.rsqrt(variance + EPS)).reshape(retained.shape[0], -1)
    scaled = scaled * group_gain[None, :] + group_bias[None, :]
    return (jax.nn.silu(gate_rows.astype(jnp.float32)) * scaled).astype(jnp.bfloat16)

def reference(hidden_states, norm_gain, query_weight, key_weight, value_weight, output_gate_weight, unit_input_weight, unit_gate_weight, decay_forward, decay_backward, group_gain, group_bias, depth_kernel, depth_bias, channel_gain, channel_bias, retention_out_weight, convolution_out_weight):
    widened = hidden_states.astype(jnp.float32)
    normed = (widened * lax.rsqrt(lax.optimization_barrier(jnp.mean(widened * widened, axis=-1, keepdims=True)) + EPS) * norm_gain[None, :]).astype(jnp.bfloat16)

    def project(weight):
        return jnp.dot(normed, weight, preferred_element_type=jnp.float32).astype(jnp.bfloat16)
    proj_q = project(query_weight)
    proj_k = project(key_weight)
    proj_v = project(value_weight)
    proj_g = project(output_gate_weight)
    proj_a = project(unit_input_weight)
    proj_b = project(unit_gate_weight)
    positions = jnp.arange(TOKENS, dtype=jnp.int32)
    queries = rotate(proj_q.reshape(TOKENS, HEADS, HEAD_DIM), positions)
    key_rows = rotate(proj_k.reshape(TOKENS, HEADS, HEAD_DIM), positions)
    values = proj_v.reshape(TOKENS, HEADS, HEAD_DIM)
    log_forward = jax.nn.log_sigmoid(decay_forward)
    log_backward = jax.nn.log_sigmoid(decay_backward)
    ahead, unused_ahead = blockwise(to_blocks(queries), to_blocks(key_rows), to_blocks(values), log_forward, True)
    behind, unused_behind = blockwise(to_blocks(queries[::-1]), to_blocks(key_rows[::-1]), to_blocks(values[::-1]), log_backward, False)
    retained = from_blocks(ahead) + from_blocks(behind)[::-1]
    retention_rows = group_norm(retained, group_gain, group_bias, proj_g)
    unit = (proj_a.astype(jnp.float32) * jax.nn.sigmoid(proj_b.astype(jnp.float32))).astype(jnp.bfloat16)
    half_kernel = (KERNEL - 1) // 2
    padded = jnp.pad(unit, ((half_kernel, half_kernel), (0, 0)))
    filtered = jnp.broadcast_to(depth_bias[None, :], (TOKENS, CONV_WIDTH))
    for offset in range(KERNEL):
        filtered = filtered + depth_kernel[offset][None, :] * padded[offset:offset + TOKENS].astype(jnp.float32)
    row_mean = lax.optimization_barrier(jnp.sum(filtered, axis=1, keepdims=True)) / CONV_WIDTH
    variance = lax.optimization_barrier(jnp.sum(filtered * filtered, axis=1, keepdims=True)) / CONV_WIDTH - row_mean * row_mean
    leveled = (filtered - row_mean) * lax.rsqrt(variance + EPS) * channel_gain[None, :] + channel_bias[None, :]
    convolution_rows = jax.nn.silu(leveled).astype(jnp.bfloat16)
    ret_group = RET_WIDTH // N_TP
    conv_group = CONV_WIDTH // N_TP
    mixed = jnp.zeros((TOKENS, D), jnp.float32)
    for group in range(N_TP):
        partial_value = jnp.dot(retention_rows[:, group * ret_group:(group + 1) * ret_group], retention_out_weight[group * ret_group:(group + 1) * ret_group], preferred_element_type=jnp.float32)
        partial_value = partial_value + jnp.dot(convolution_rows[:, group * conv_group:(group + 1) * conv_group], convolution_out_weight[group * conv_group:(group + 1) * conv_group], preferred_element_type=jnp.float32)
        rounded = lax.optimization_barrier(partial_value.astype(jnp.bfloat16))
        mixed = mixed + rounded.astype(jnp.float32)
    return mixed.astype(jnp.bfloat16)
```

```python
import functools

import jax
import jax.numpy as jnp
from jax import lax
from jax.experimental import pallas as pl
from jax.experimental.pallas import tpu as pltpu
from jax.sharding import PartitionSpec as P

HEAD_DIM = 128
CONV_WIDTH = 2048
KERNEL = 31
EPS = 1e-06
THETA = 10000.0
ROWS = 512
BF = jnp.bfloat16
F32 = jnp.float32
MESH = pl.DeviceIdType.MESH
VM = pl.BlockSpec(memory_space=pltpu.VMEM)
ANY = pl.BlockSpec(memory_space=pl.ANY)
MIB = 1 << 20


def place():
    sp, tp = lax.axis_index("sp"), lax.axis_index("tp")
    return tp // 2, sp % 4, sp // 4, tp % 2


def at(x, y, z, c):
    return (z * 4 + y, x * 2 + c)


def when(cond, f):
    if cond is None:
        f()
    else:
        pl.when(cond)(f)


class Post:
    def __init__(self, send_sems, recv_sems):
        self.ss, self.rs = send_sems, recv_sems
        self.sent, self.ids = [], {}

    def key(self, name):
        return self.rs.at[self.ids.setdefault(name, len(self.ids))]

    def send(self, name, src, dst, to, cond=None):
        sem, recv = self.ss.at[len(self.sent)], self.key(name)

        def make():
            return pltpu.make_async_remote_copy(
                src_ref=src, dst_ref=dst, send_sem=sem, recv_sem=recv, device_id=to, device_id_type=MESH
            )

        self.sent.append((make, cond))
        when(cond, lambda: make().start())

    def local(self, name, src, dst, cond=None):
        recv = self.key(name)
        when(cond, lambda: pltpu.make_async_copy(src, dst, recv).start())

    def recv(self, name, ref, cond=None):
        recv = self.key(name)
        when(cond, lambda: pltpu.make_async_copy(ref, ref, recv).wait())

    def finish(self):
        for make, cond in self.sent:
            when(cond, lambda: make().wait_send())


def greet(peers):
    barrier = pltpu.get_barrier_semaphore()
    for peer in peers:
        pl.semaphore_signal(barrier, inc=1, device_id=peer, device_id_type=MESH)
    pl.semaphore_wait(barrier, len(peers))


def rows_at(start, size, unit=16):
    return pl.ds(pl.multiple_of(start, unit), size)


def cols_at(start, size):
    return pl.ds(pl.multiple_of(start, 128), size)


def gather_kernel(xin, wq, wk, wv, wg, wa, wb, wr, wc, par, xg, wt, wo, pg, ss, rs):
    x, y, z, c = place()
    ct, yl = y // 2, y % 2
    xp, xm, x2 = (x + 1) % 4, (x + 3) % 4, (x + 2) % 4
    yp, ym, y2 = (y + 1) % 4, (y + 3) % 4, (y + 2) % 4
    zp, zm = (z + 1) % 8, (z + 7) % 8
    own = ct == c
    other = ct != c
    post = Post(ss, rs)
    partner = at(x, y, z, 1 - c)
    greet(
        [at(q, y, z, k) for q in (xp, xm) for k in (0, 1)]
        + [at(x, q, z, k) for q in (yp, ym, y2) for k in (0, 1)]
        + [at(x, y, zp, c), at(x, y, zm, c), partner]
    )

    def xblock(yy, half, r0, rn, col, width):
        return xg.at[rows_at((yy % 2) * 256 + half * 128 + r0, rn), cols_at(col, width)]

    mine = (x * 2 + c) * 512
    for half, name, ends in ((0, "x1", ((xp, y, "m"), (xm, y, "p"))), (1, "x2", ((x, yp, "m"), (x, ym, "p")))):
        src, dst = xin.at[pl.ds(half * 128, 128), :], xblock(y, half, 0, 128, mine, 512)
        for qx, qy, d in ends:
            post.send(name + d, src, dst, at(qx, qy, z, ct))
        post.send(name + "l", src, dst, partner, other)
        post.local(name + "s", src, dst, own)

    s = z * 4 + y
    for j in (0, 1):
        q = 2 * c + j
        here = (q == y) & own
        away = jnp.logical_not(here)
        to = at(x, q, z, ct)
        for m, w in enumerate((wq, wk, wv, wg, wa, wb)):
            src, dst = w.at[:, pl.ds(j * 128, 128)], wt.at[rows_at(s * 128, 128), pl.ds(m * 128, 128)]
            post.send("w", src, dst, to, away)
            post.local("w", src, dst, here)
    for j in (0, 1):
        q = 2 * c + j
        here = (q == y) & own
        away = jnp.logical_not(here)
        to = at(x, q, z, ct)
        for m, w in enumerate((wr, wc)):
            src, dst = w.at[pl.ds(j * 128, 128), :], wo.at[pl.ds(m * 128, 128), cols_at(s * 128, 128)]
            post.send("o", src, dst, to, away)
            post.local("o", src, dst, here)
    src = par.at[:, cols_at(yl * 128, 128)]
    post.send("par", src, pg, partner, own)
    post.local("pars", src, pg, own)

    def wrows(zz, u, n=1):
        return wt.at[rows_at((zz * 4 + 2 * c + u) * 128, 128 * n), :]

    def zsend(zz, u, r, d):
        ref = wrows(zz, u)
        post.send(("z", d, r, u), ref, ref, at(x, y, zp if d == "m" else zm, c))

    def zpass(zz, u, rel):
        ref = wrows(zz, u)
        post.send(("zp", rel, u), ref, ref, partner)

    def ocols(zz, core=c, r0=0, rn=256):
        return wo.at[pl.ds(r0, rn), cols_at((zz * 4 + 2 * core) * 128, 256)]

    def osend(zz, r, d, r0=0, rn=256):
        ref = ocols(zz, c, r0, rn)
        post.send(("o", d, r), ref, ref, at(x, y, zp if d == "m" else zm, c))

    def opass(zz, rel, r0=0, rn=256):
        ref = ocols(zz, c, r0, rn)
        post.send(("op", rel, r0), ref, ref, partner)

    post.recv("w", wrows(z, 0, 2))
    for d, order in (("m", (0, 1)), ("p", (1, 0))):
        for u in order:
            zsend(z, u, 1, d)
    for u in (0, 1):
        zpass(z, u, 0)

    cm, cp, c2 = ym // 2 == c, yp // 2 == c, y2 // 2 == c
    post.recv("x1m", xblock(y, 0, 0, 128, xm * 1024, 1024), own)
    ref = xblock(y, 0, 0, 64, xm * 1024, 1024)
    post.send("x1m2", ref, ref, at(xp, y, z, c), own)
    post.recv("x1p", xblock(y, 0, 0, 128, xp * 1024, 1024), own)
    ref = xblock(y, 0, 64, 64, xp * 1024, 1024)
    post.send("x1p2", ref, ref, at(xm, y, z, c), own)
    post.recv("x2m", xblock(ym, 1, 0, 128, x * 1024, 1024), cm)
    ref = xblock(ym, 1, 0, 64, x * 1024, 1024)
    post.send("x2m2", ref, ref, at(x, yp, z, c), cm)
    post.recv("x2p", xblock(yp, 1, 0, 128, x * 1024, 1024), cp)
    ref = xblock(yp, 1, 64, 64, x * 1024, 1024)
    post.send("x2p2", ref, ref, at(x, ym, z, c), cp)

    for name, half in (("x1", 0), ("x2", 1)):
        block = xblock(y, half, 0, 128, mine, 512)
        post.recv(name + "s", block, own)
        post.recv(name + "l", xblock(y, half, 0, 128, (x * 2 + 1 - c) * 512, 512), own)
    post.recv("x1m2", xblock(y, 0, 0, 64, x2 * 1024, 1024), own)
    post.recv("x1p2", xblock(y, 0, 64, 64, x2 * 1024, 1024), own)
    for u in (0, 1):
        ref = xblock(y, 0, u * 64, 64, 0, 4096)
        post.send(("x3m", u), ref, ref, at(x, yp, z, c), own)
    for u in (1, 0):
        ref = xblock(y, 0, u * 64, 64, 0, 4096)
        post.send(("x3p", u), ref, ref, at(x, ym, z, c), own)
    post.recv("x2m2", xblock(y2, 1, 0, 64, x * 1024, 1024), c2)
    post.recv("x2p2", xblock(y2, 1, 64, 64, x * 1024, 1024), c2)

    def x4(qx, k):
        return xblock(k, 1, 0, 128, qx * 1024, 1024)

    for d, to, order in (("m", xp, (0, 1)), ("p", xm, (1, 0))):
        for k in order:
            post.send(("x4" + d, k), x4(x, k), x4(x, k), at(to, y, z, c))

    def zstep(r):
        for i in (0, 1):
            for d, u in (("m", i), ("p", 1 - i)):
                zz = (z - r) % 8 if d == "m" else (z + r) % 8
                post.recv(("z", d, r, u), wrows(zz, u))
                if r < 3 or i == 0:
                    zsend(zz, u, r + 1, d)
                zpass(zz, u, -r % 8 if d == "m" else r)

    zstep(1)
    post.recv(("x3m", 0), xblock(ym, 0, 0, 64, 0, 4096), cm)
    ref = xblock(ym, 0, 0, 64, 0, 4096)
    post.send("x3m2", ref, ref, at(x, yp, z, c), cm)
    post.recv(("x3p", 1), xblock(yp, 0, 64, 64, 0, 4096), cp)
    ref = xblock(yp, 0, 64, 64, 0, 4096)
    post.send("x3p2", ref, ref, at(x, ym, z, c), cp)
    post.recv(("x4m", 0), x4(xm, 0))
    post.send("x4m2", x4(xm, 0), x4(xm, 0), at(xp, y, z, c))
    post.recv(("x4p", 1), x4(xp, 1))
    post.send("x4p2", x4(xp, 1), x4(xp, 1), at(xm, y, z, c))
    zstep(2)
    post.recv("o", ocols(z))
    zstep(3)
    for d in ("m", "p"):
        osend(z, 1, d)
    opass(z, 0)
    for d, u in (("m", 0), ("p", 1)):
        post.recv(("z", d, 4, u), wrows((z + 4) % 8, u))
        zpass((z + 4) % 8, u, 4)
    for r in (1, 2, 3):
        for d in ("m", "p"):
            zz = (z - r) % 8 if d == "m" else (z + r) % 8
            post.recv(("o", d, r), ocols(zz))
            if r < 3:
                osend(zz, r + 1, d)
            else:
                osend(zz, 4, d, 0 if d == "m" else 128, 128)
            opass(zz, -r % 8 if d == "m" else r)
    for d, r0 in (("m", 0), ("p", 128)):
        post.recv(("o", d, 4), ocols((z + 4) % 8, c, r0, 128))
        opass((z + 4) % 8, 4, r0, 128)

    post.recv("pars", pg, own)
    post.recv("par", pg, other)
    post.recv(("x3m", 1), xblock(ym, 0, 64, 64, 0, 4096), cm)
    post.recv(("x3p", 0), xblock(yp, 0, 0, 64, 0, 4096), cp)
    post.recv("x3m2", xblock(y2, 0, 0, 64, 0, 4096), c2)
    post.recv("x3p2", xblock(y2, 0, 64, 64, 0, 4096), c2)
    post.recv(("x4m", 1), x4(xm, 1))
    post.recv(("x4p", 0), x4(xp, 0))
    post.recv("x4m2", x4(x2, 0))
    post.recv("x4p2", x4(x2, 1))
    for rel in range(8):
        zz = (z + rel) % 8
        for u in (0, 1):
            ref = wt.at[rows_at((zz * 4 + 2 * (1 - c) + u) * 128, 128), :]
            post.recv(("zp", rel, u), ref)
        if rel == 4:
            for r0 in (0, 128):
                post.recv(("op", rel, r0), ocols(zz, 1 - c, r0, 128))
        else:
            post.recv(("op", rel, 0), ocols(zz, 1 - c))
    post.finish()


def gather(xin, weights, outs, par):
    return pl.pallas_call(
        gather_kernel,
        name="gather",
        out_shape=(
            jax.ShapeDtypeStruct((ROWS, 4096), BF),
            jax.ShapeDtypeStruct((4096, 768), BF),
            jax.ShapeDtypeStruct((256, 4096), BF),
            jax.ShapeDtypeStruct((40, 128), F32),
        ),
        in_specs=[ANY] * 10,
        out_specs=(VM,) * 4,
        scratch_shapes=[pltpu.SemaphoreType.DMA((128,)), pltpu.SemaphoreType.DMA((96,))],
        compiler_params=pltpu.CompilerParams(
            collective_id=0, has_side_effects=True, vmem_limit_bytes=32 * MIB
        ),
    )(xin, *weights, *outs, par)


def dot(a, b, dims=((1,), (0,))):
    return lax.dot_general(a, b, (dims, ((), ())), preferred_element_type=F32)


def project_kernel(xg, wt, pg, gain, cosine, sine, q_ref, in_ref, g_ref, u_ref, st_ref, nrm):
    @pl.loop(0, ROWS // 128)
    def _(i):
        rows = rows_at(i * 128, 128)
        square = jnp.zeros((128, 128), F32)
        for k in range(32):
            part = xg[rows, k * 128 : k * 128 + 128].astype(F32)
            square = square + part * part
        scale = lax.rsqrt(jnp.sum(square, axis=1, keepdims=True) / 4096 + EPS)
        for k in range(32):
            cols = slice(k * 128, k * 128 + 128)
            nrm[rows, cols] = (xg[rows, cols].astype(F32) * scale * gain[:, cols]).astype(BF)

    proj = dot(nrm[...], wt[...]).astype(BF)

    def turn(rows):
        wide = rows.astype(F32)
        return (wide * cosine[...] + pltpu.roll(wide, 64, axis=1) * sine[...]).astype(BF)

    queries, keys = turn(proj[:, 0:128]), turn(proj[:, 128:256])
    values = proj[:, 256:384]
    q_ref[...] = queries
    g_ref[...] = proj[:, 384:512]
    u_ref[...] = (proj[:, 512:640].astype(F32) * jax.nn.sigmoid(proj[:, 640:768].astype(F32))).astype(BF)
    lf, lb = pg[36:37, :], pg[37:38, :]
    place_ = lax.broadcasted_iota(jnp.int32, (ROWS, 128), 0).astype(F32)
    wide = keys.astype(F32)
    st_ref[0] = dot((wide * jnp.exp(lb * place_)).astype(BF), values, ((0,), (0,))).astype(BF)
    st_ref[1] = dot((wide * jnp.exp(lf * (ROWS - 1.0 - place_))).astype(BF), values, ((0,), (0,))).astype(BF)
    f1, b1 = lf[:, 0:1], lb[:, 0:1]
    for i in range(ROWS // 128):
        rows = slice(i * 128, i * 128 + 128)
        gap = (
            lax.broadcasted_iota(jnp.int32, (128, ROWS), 0)
            + i * 128
            - lax.broadcasted_iota(jnp.int32, (128, ROWS), 1)
        ).astype(F32)
        decay = jnp.exp(jnp.where(gap >= 0, f1 * gap, -b1 * gap))
        scores = dot(queries[rows], keys, ((1,), (1,))) * decay
        in_ref[rows, :] = dot(scores.astype(BF), values)


def project(xg, wt, pg, gain, cosine, sine):
    small = jax.ShapeDtypeStruct((ROWS, 128), BF)
    return pl.pallas_call(
        project_kernel,
        name="project",
        out_shape=(
            small,
            jax.ShapeDtypeStruct((ROWS, 128), F32),
            small,
            small,
            jax.ShapeDtypeStruct((2, 128, 128), BF),
        ),
        in_specs=[VM] * 6,
        out_specs=(VM,) * 5,
        scratch_shapes=[pltpu.VMEM((ROWS, 4096), BF)],
        compiler_params=pltpu.CompilerParams(vmem_limit_bytes=40 * MIB),
    )(xg, wt, pg, gain, cosine, sine)


def states_kernel(st, unit, sg, halo, ss, rs):
    x, y, z, c = place()
    n = z * 2 + c
    post = Post(ss, rs)
    peers = []
    for dz in range(8):
        for k in (0, 1):
            if dz or k:
                n2 = ((z + dz) % 8) * 2 + (c + k) % 2
                peers.append((n2, at(x, y, n2 // 2, n2 % 2)))
    greet([peer for _, peer in peers])
    after, before = (n + 1) % 16, (n + 15) % 16
    post.send("ht", unit.at[pl.ds(ROWS - 16, 16), :], halo.at[0], at(x, y, after // 2, after % 2))
    post.send("hh", unit.at[pl.ds(0, 16), :], halo.at[1], at(x, y, before // 2, before % 2))
    for n2, peer in peers:
        post.send("st", st.at[(n2 - n + 16) // 16], sg.at[n], peer)
    sg[pl.ds(n, 1)] = jnp.zeros((1, 128, 128), BF)
    post.recv("ht", halo.at[0])
    post.recv("hh", halo.at[1])
    post.recv("st", sg.at[pl.ds(0, 15)])
    post.finish()


def exchange_states(st, unit):
    return pl.pallas_call(
        states_kernel,
        name="states",
        out_shape=(jax.ShapeDtypeStruct((16, 128, 128), BF), jax.ShapeDtypeStruct((2, 16, 128), BF)),
        in_specs=[VM] * 2,
        out_specs=(VM,) * 2,
        scratch_shapes=[pltpu.SemaphoreType.DMA((17,)), pltpu.SemaphoreType.DMA((3,))],
        compiler_params=pltpu.CompilerParams(
            collective_id=1, has_side_effects=True, vmem_limit_bytes=8 * MIB
        ),
    )(st, unit)


def middle_kernel(q_ref, in_ref, g_ref, u_ref, sg, halo, pg, rows_ref, filt_ref, stat_ref, pad):
    x, y, z, c = place()
    n = z * 2 + c
    lf, lb = pg[36:37, :], pg[37:38, :]
    enter_f, enter_b = jnp.zeros((128, 128), F32), jnp.zeros((128, 128), F32)
    for j in range(16):
        state = sg[j].astype(F32)
        ahead, behind = n - 1 - j, j - n - 1
        wf = jnp.exp(lf * (ROWS * jnp.maximum(ahead, 0)).astype(F32))
        wb = jnp.exp(lb * (ROWS * jnp.maximum(behind, 0)).astype(F32))
        enter_f = enter_f + jnp.where(ahead >= 0, wf, 0.0) * state
        enter_b = enter_b + jnp.where(behind >= 0, wb, 0.0) * state
    place_ = lax.broadcasted_iota(jnp.int32, (ROWS, 128), 0).astype(F32)
    wide = q_ref[...].astype(F32)
    retained = in_ref[...]
    retained = retained + dot((wide * jnp.exp(lf * (place_ + 1.0))).astype(BF), enter_f.astype(BF))
    retained = retained + dot((wide * jnp.exp(lb * (ROWS - place_))).astype(BF), enter_b.astype(BF))
    mean = jnp.mean(retained, axis=-1, keepdims=True)
    centered = retained - mean
    variance = jnp.mean(centered * centered, axis=-1, keepdims=True)
    scaled = centered * lax.rsqrt(variance + EPS) * pg[34:35, :] + pg[35:36, :]
    rows_ref[...] = (jax.nn.silu(g_ref[...].astype(F32)) * scaled).astype(BF)

    pad[0:16, :] = jnp.where(n > 0, halo[0].astype(F32), 0.0)
    pad[16 : 16 + ROWS, :] = u_ref[...].astype(F32)
    pad[16 + ROWS :, :] = jnp.where(n < 15, halo[1].astype(F32), 0.0)
    lane = lax.broadcasted_iota(jnp.int32, (128, 128), 1)
    for i in range(ROWS // 128):
        filtered = jnp.broadcast_to(pg[31:32, :], (128, 128))
        for t in range(KERNEL):
            filtered = filtered + pg[t : t + 1, :] * pad[i * 128 + t + 1 : i * 128 + t + 129, :]
        filt_ref[i * 128 : i * 128 + 128, :] = filtered
        total = jnp.sum(filtered, axis=1, keepdims=True)
        square = jnp.sum(filtered * filtered, axis=1, keepdims=True)
        tile = jnp.where(lane == 0, total, jnp.where(lane == 1, square, 0.0))
        stat_ref[:, i * 128 : i * 128 + 128] = tile.T[0:8, :]


def middle(queries, inner, gates, unit, sg, halo, pg):
    return pl.pallas_call(
        middle_kernel,
        name="middle",
        out_shape=(
            jax.ShapeDtypeStruct((ROWS, 128), BF),
            jax.ShapeDtypeStruct((ROWS, 128), F32),
            jax.ShapeDtypeStruct((8, ROWS), F32),
        ),
        in_specs=[VM] * 7,
        out_specs=(VM,) * 3,
        scratch_shapes=[pltpu.VMEM((ROWS + 32, 128), F32)],
        compiler_params=pltpu.CompilerParams(vmem_limit_bytes=16 * MIB),
    )(queries, inner, gates, unit, sg, halo, pg)


def stats_kernel(st, all_, ss, rs):
    x, y, z, c = place()
    me = x * 4 + y
    post = Post(ss, rs)
    peers = [at((x + i) % 4, (y + j) % 4, z, c) for i in range(4) for j in range(4) if i or j]
    greet(peers)
    for peer in peers:
        post.send("s", st, all_.at[me], peer)
    all_[pl.ds(me, 1)] = st[...][None]
    post.recv("s", all_.at[pl.ds(0, 15)])
    post.finish()


def exchange_stats(st):
    return pl.pallas_call(
        stats_kernel,
        name="stats",
        out_shape=jax.ShapeDtypeStruct((16, 8, ROWS), F32),
        in_specs=[VM],
        out_specs=VM,
        scratch_shapes=[pltpu.SemaphoreType.DMA((15,)), pltpu.SemaphoreType.DMA((1,))],
        compiler_params=pltpu.CompilerParams(
            collective_id=2, has_side_effects=True, vmem_limit_bytes=8 * MIB
        ),
    )(st)


def out_kernel(rows_ref, filt_ref, stats, pg, wo, part_ref):
    total = stats[0]
    for j in range(1, 16):
        total = total + stats[j]
    for i in range(ROWS // 128):
        rows = slice(i * 128, i * 128 + 128)
        tall = jnp.concatenate([total[:, rows], jnp.zeros((120, 128), F32)], axis=0).T
        mean = tall[:, 0:1] / CONV_WIDTH
        variance = tall[:, 1:2] / CONV_WIDTH - mean * mean
        leveled = (filt_ref[rows, :] - mean) * lax.rsqrt(variance + EPS) * pg[32:33, :] + pg[33:34, :]
        both = jnp.concatenate([rows_ref[rows, :], jax.nn.silu(leveled).astype(BF)], axis=1)
        for k in range(8):
            cols = slice(k * 512, k * 512 + 512)
            part_ref[rows, cols] = dot(both, wo[:, cols]).astype(BF)


def out_part(ret_rows, filtered, stats, pg, wo):
    return pl.pallas_call(
        out_kernel,
        name="outpart",
        out_shape=jax.ShapeDtypeStruct((ROWS, 4096), BF),
        in_specs=[VM] * 5,
        out_specs=VM,
        compiler_params=pltpu.CompilerParams(vmem_limit_bytes=24 * MIB),
    )(ret_rows, filtered, stats, pg, wo)


def scatter_kernel(part, out, a2m, a2p, am, ap, ta, u, ua, b2m, b2p, bm, bp, bo, tb, v, vb, ss, rs):
    x, y, z, c = place()
    xp, xm, x2 = (x + 1) % 4, (x + 3) % 4, (x + 2) % 4
    yp, ym, y2 = (y + 1) % 4, (y + 3) % 4, (y + 2) % 4
    post = Post(ss, rs)
    partner = at(x, y, z, 1 - c)
    greet(
        [at(q, y, z, c) for q in (xp, xm, x2)]
        + [at(x, q, z, k) for q in (yp, ym, y2) for k in (0, 1)]
        + [partner]
    )
    left, right = pl.ds(0, 2048), pl.ds(2048, 2048)
    own, other = y // 2 == c, y // 2 != c
    c1p, c1m, c2 = yp // 2 == c, ym // 2 == c, y2 // 2 == c
    to_xp, to_xm = at(xp, y, z, c), at(xm, y, z, c)

    def pa(k, q):
        return part.at[k, q, :, :, left]

    def pb(yy, q0, k):
        return part.at[yy % 2, pl.ds(q0, 2), k, :, right]

    post.send("a2m", pa(0, x2), a2m, to_xp)
    post.send("a2p", pa(1, x2), a2p, to_xm)
    for k in (0, 1):
        post.send("b2m", pb(y2, 0, k), b2m.at[k], at(x, yp, z, c), c2)
        post.send("b2p", pb(y2, 2, k), b2p.at[k], at(x, ym, z, c), c2)
    post.send("am1", pa(1, xp), am.at[1], to_xp)
    post.send("ap0", pa(0, xm), ap.at[0], to_xm)
    for k in (0, 1):
        post.send("bm1", pb(yp, 2, k), bm.at[pl.ds(2, 2)], at(x, yp, z, k), c1p)
        post.send("bp0", pb(ym, 0, k), bp.at[pl.ds(0, 2)], at(x, ym, z, k), c1m)
    post.send("bo", part.at[y % 2, :, 1 - c, :, right], bo, partner, own)

    def add(a, b):
        return (a.astype(F32) + b.astype(F32)).astype(BF)

    post.recv("a2m", a2m)
    ta[0] = add(a2m[...], part[0, xp, :, :, 0:2048])
    post.send("am0", ta.at[0], am.at[0], to_xp)
    post.recv("a2p", a2p)
    ta[1] = add(a2p[...], part[1, xm, :, :, 0:2048])
    post.send("ap1", ta.at[1], ap.at[1], to_xm)

    post.recv("b2m", b2m, c1p)

    @pl.when(c1p)
    def _():
        for k in (0, 1):
            tb[0, k] = add(b2m[k], part[yp % 2, 0:2, k, :, 2048:4096])

    for k in (0, 1):
        post.send("bm0", tb.at[0, k], bm.at[pl.ds(0, 2)], at(x, yp, z, k), c1p)
    post.recv("b2p", b2p, c1m)

    @pl.when(c1m)
    def _():
        for k in (0, 1):
            tb[1, k] = add(b2p[k], part[ym % 2, 2:4, k, :, 2048:4096])

    for k in (0, 1):
        post.send("bp1", tb.at[1, k], bp.at[pl.ds(2, 2)], at(x, ym, z, k), c1m)

    @pl.when(own)
    def _():
        bo[...] = part[y % 2, :, c, :, 2048:4096]

    post.recv("am1", am.at[1])
    post.recv("ap0", ap.at[0])
    post.recv("am0", am.at[0])
    post.recv("ap1", ap.at[1])
    for k in (0, 1):
        u[k] = (part[k, x, :, :, 0:2048].astype(F32) + am[k].astype(F32) + ap[k].astype(F32)).astype(BF)
    for k in (0, 1):
        for k2 in (0, 1):
            q = 2 * c + k
            here = (q == y) & (k2 == c)
            post.send("ua", u.at[k, k2], ua.at[y], at(x, q, z, k2), jnp.logical_not(here))
            post.local("ua", u.at[k, k2], ua.at[y], here)
    post.recv("bm1", bm.at[pl.ds(2, 2)])
    post.recv("bp0", bp.at[pl.ds(0, 2)])
    post.recv("bo", bo, other)
    post.recv("bm0", bm.at[pl.ds(0, 2)])
    post.recv("bp1", bp.at[pl.ds(2, 2)])
    for q in range(4):
        v[q] = (bm[q].astype(F32) + bp[q].astype(F32) + bo[q].astype(F32)).astype(BF)
    for d, q in (("2", x2), ("p", xp), ("m", xm)):
        post.send("vb", v.at[q], vb.at[x], at(q, y, z, c))
    post.recv("ua", ua)
    out[:, 0:2048] = (
        ua[0].astype(F32) + ua[1].astype(F32) + ua[2].astype(F32) + ua[3].astype(F32)
    ).astype(BF)
    vb[pl.ds(x, 1)] = v[pl.ds(x, 1)]
    post.recv("vb", vb.at[pl.ds(0, 3)])
    out[:, 2048:4096] = (
        vb[0].astype(F32) + vb[1].astype(F32) + vb[2].astype(F32) + vb[3].astype(F32)
    ).astype(BF)
    post.finish()


def scatter(part):
    buf = lambda *shape: pltpu.VMEM((*shape, 2048), BF)
    return pl.pallas_call(
        scatter_kernel,
        name="scatter",
        out_shape=jax.ShapeDtypeStruct((32, 4096), BF),
        in_specs=[VM],
        out_specs=VM,
        scratch_shapes=[
            buf(2, 32),
            buf(2, 32),
            buf(2, 2, 32),
            buf(2, 2, 32),
            buf(2, 2, 32),
            buf(2, 2, 32),
            buf(4, 32),
            buf(2, 2, 32),
            buf(2, 2, 32),
            buf(4, 32),
            buf(4, 32),
            buf(4, 32),
            buf(2, 2, 2, 32),
            buf(4, 32),
            buf(4, 32),
            pltpu.SemaphoreType.DMA((32,)),
            pltpu.SemaphoreType.DMA((16,)),
        ],
        compiler_params=pltpu.CompilerParams(
            collective_id=3, has_side_effects=True, vmem_limit_bytes=24 * MIB
        ),
    )(part.reshape(2, 4, 2, 32, 4096))


def shards(
    hidden_states,
    norm_gain,
    query_weight,
    key_weight,
    value_weight,
    output_gate_weight,
    unit_input_weight,
    unit_gate_weight,
    decay_forward,
    decay_backward,
    group_gain,
    group_bias,
    depth_kernel,
    depth_bias,
    channel_gain,
    channel_bias,
    retention_out_weight,
    convolution_out_weight,
):
    x, y, z, c = place()
    spread = lambda decay: jnp.repeat(jax.nn.log_sigmoid(decay), HEAD_DIM)
    par = jnp.concatenate(
        [
            depth_kernel,
            jnp.stack(
                [
                    depth_bias,
                    channel_gain,
                    channel_bias,
                    group_gain,
                    group_bias,
                    spread(decay_forward),
                    spread(decay_backward),
                ]
            ),
            jnp.zeros((2, 256), F32),
        ]
    )
    half = HEAD_DIM // 2
    positions = (z * 2 + c) * ROWS + jnp.arange(ROWS, dtype=jnp.int32)
    inverse = THETA ** (-jnp.arange(half, dtype=F32) / half)
    angles = positions.astype(F32)[:, None] * inverse[None, :]
    cosine, sine = jnp.cos(angles), jnp.sin(angles)
    cosine = jnp.concatenate([cosine, cosine], axis=1)
    sine = jnp.concatenate([-sine, sine], axis=1)

    xg, wt, wo, pg = gather(
        hidden_states,
        (query_weight, key_weight, value_weight, output_gate_weight, unit_input_weight, unit_gate_weight),
        (retention_out_weight, convolution_out_weight),
        par,
    )
    queries, inner, gates, unit, st = project(xg, wt, pg, norm_gain[None, :], cosine, sine)
    sg, halo = exchange_states(st, unit)
    ret_rows, filtered, stat = middle(queries, inner, gates, unit, sg, halo, pg)
    stats = exchange_stats(stat)
    return scatter(out_part(ret_rows, filtered, stats, pg, wo))


def solution(mesh):
    split = P("sp", "tp")
    placed = (
        (split, P())
        + (split,) * 6
        + (P("tp"),) * 4
        + (P(None, "tp"),)
        + (P("tp"),) * 3
        + (P("tp", "sp"),) * 2
    )
    return jax.shard_map(
        shards, mesh=mesh, in_specs=placed, out_specs=P(("sp", "tp"), None), check_vma=False
    )
```

```python
import functools

import jax
import jax.numpy as jnp
import numpy as np
from jax import lax
from jax.experimental import pallas as pl
from jax.experimental.pallas import tpu as pltpu
from jax.sharding import PartitionSpec as P

HEAD_DIM = 128
CONV_WIDTH = 2048
KERNEL = 31
EPS = 1e-06
THETA = 10000.0
ROWS = 512
BF = jnp.bfloat16
F32 = jnp.float32
MESH = pl.DeviceIdType.MESH
VM = pl.BlockSpec(memory_space=pltpu.VMEM)
HBM = pl.BlockSpec(memory_space=pltpu.HBM)
SM = pl.BlockSpec(memory_space=pltpu.SMEM)
MIB = 1 << 20


def place():
    sp, tp = lax.axis_index("sp"), lax.axis_index("tp")
    return tp // 2, sp % 4, sp // 4, tp % 2


def at(x, y, z, c):
    return (z * 4 + y, x * 2 + c)


def when(cond, f):
    if cond is None:
        f()
    else:
        pl.when(cond)(f)


class Post:
    def __init__(self, send_sems, recv_sems):
        self.ss, self.rs = send_sems, recv_sems
        self.sent, self.ids = [], {}

    def key(self, name):
        return self.rs.at[self.ids.setdefault(name, len(self.ids))]

    def send(self, name, src, dst, to, cond=None, recv=None):
        sem = self.ss.at[len(self.sent)]
        recv = self.key(name) if recv is None else recv

        def make():
            return pltpu.make_async_remote_copy(
                src_ref=src, dst_ref=dst, send_sem=sem, recv_sem=recv, device_id=to, device_id_type=MESH
            )

        self.sent.append((make, cond))
        when(cond, lambda: make().start())

    def local(self, name, src, dst, cond=None, recv=None):
        recv = self.key(name) if recv is None else recv
        when(cond, lambda: pltpu.make_async_copy(src, dst, recv).start())

    def recv(self, name, ref, cond=None, recv=None):
        recv = self.key(name) if recv is None else recv
        when(cond, lambda: pltpu.make_async_copy(ref, ref, recv).wait())

    def finish(self):
        for make, cond in self.sent:
            when(cond, lambda: make().wait_send())


def greet(peers):
    barrier = pltpu.get_barrier_semaphore()
    for peer in peers:
        pl.semaphore_signal(barrier, inc=1, device_id=peer, device_id_type=MESH)
    pl.semaphore_wait(barrier, len(peers))


def rows_at(start, size, unit=16):
    return pl.ds(pl.multiple_of(start, unit), size)


def cols_at(start, size):
    return pl.ds(pl.multiple_of(start, 128), size)


def dot(a, b, dims=((1,), (0,))):
    return lax.dot_general(a, b, (dims, ((), ())), preferred_element_type=F32)


def log_sigmoid(decay):
    t = jnp.exp(-decay)
    s = t / (2.0 + t)
    square = s * s
    series = jnp.full_like(s, 1.0 / 15)
    for n in (13, 11, 9, 7, 5, 3, 1):
        series = series * square + 1.0 / n
    return -2.0 * s * series


def mixer_kernel(
    xin, wq, wk, wv, wg, wa, wb, wr, wc, dk_in, pv_in, gain_in, cos_in, sin_in, base_in, df, db, out,
    xg, nrm, wt, wo, dk, pv, gain, cosine, sine, base, dec, decp, qs, inner, gs, us, st, sg, halo,
    pad, filt, stat, stats, both, part,
    a2m, a2p, am, ap, ta, u, ua, b2m, b2p, bm, bp, bo, tb, v, vb, ss, rs,
):
    x, y, z, c = place()
    n = z * 2 + c
    ct, yl = y // 2, y % 2
    xp, xm, x2 = (x + 1) % 4, (x + 3) % 4, (x + 2) % 4
    yp, ym, y2 = (y + 1) % 4, (y + 3) % 4, (y + 2) % 4
    zp, zm = (z + 1) % 8, (z + 7) % 8
    own = ct == c
    other = ct != c
    post = Post(ss, rs)
    partner = at(x, y, z, 1 - c)
    post.local("gain", gain_in, gain)
    post.local("cos", cos_in, cosine)
    post.local("sin", sin_in, sine)
    post.local("base", base_in, base)
    line = [(dz, (z + dz) % 8) for dz in range(1, 8)]
    greet(
        [at(x, y, q, k) for _, q in line for k in (0, 1)]
        + [partner]
        + [at((x + i) % 4, (y + j) % 4, z, c) for i in range(4) for j in range(4) if i or j]
        + [at(q, y, z, 1 - c) for q in (xp, xm)]
        + [at(x, q, z, 1 - c) for q in (yp, ym, y2)]
    )

    def xblock(yy, half, r0, rn, col, width):
        return xg.at[rows_at((yy % 2) * 256 + half * 128 + r0, rn), cols_at(col, width)]

    s = z * 4 + y
    post.key("w0"), post.key("w1")
    wsem = rs.at[post.ids["w0"] + yl]
    for j in (0, 1):
        q = 2 * c + j
        here = (q == y) & own
        away = jnp.logical_not(here)
        to = at(x, q, z, ct)
        for m, w in enumerate((wq, wk, wv, wg, wa, wb)):
            src, dst = w.at[:, pl.ds(j * 128, 128)], wt.at[rows_at(s * 128, 128), pl.ds(m * 128, 128)]
            post.local("w", src, dst, here, wsem)
            post.send("w", src, dst, to, away, wsem)

    mine = (x * 2 + c) * 512
    for half, name, ends in ((0, "x1", ((xp, y, "m"), (xm, y, "p"))), (1, "x2", ((x, yp, "m"), (x, ym, "p")))):
        src, dst = xin.at[pl.ds(half * 128, 128), :], xblock(y, half, 0, 128, mine, 512)
        for qx, qy, d in ends:
            post.send(name + d, src, dst, at(qx, qy, z, ct))
        post.send(name + "l", src, dst, partner, other)
        post.local(name + "s", src, dst, own)

    for j in (0, 1):
        q = 2 * c + j
        here = (q == y) & own
        away = jnp.logical_not(here)
        to = at(x, q, z, ct)
        for m, w in enumerate((wr, wc)):
            src, dst = w.at[pl.ds(j * 128, 128), :], wo.at[pl.ds(m * 128, 128), cols_at(s * 128, 128)]
            post.send("o", src, dst, to, away)
            post.local("o", src, dst, here)
    for name, ref, dst in (("dk", dk_in, dk), ("pv", pv_in, pv)):
        src = ref.at[:, cols_at(yl * 128, 128)]
        post.send(name, src, dst, partner, own)
        post.local(name, src, dst, own)
    decp[0:1, :] = log_sigmoid(jnp.full((1, 128), df[yl], F32))
    decp[1:2, :] = log_sigmoid(jnp.full((1, 128), db[yl], F32))

    def wrows(zz, i, r0=0, rn=128):
        sub = yl if i == 0 else 1 - yl
        return wt.at[rows_at((zz * 4 + 2 * c + sub) * 128 + r0, rn), :]

    def zsend(zz, i, r, d, r0=0, rn=128):
        ref = wrows(zz, i, r0, rn)
        post.send(("z", d, r, i), ref, ref, at(x, y, zp if d == "m" else zm, c))

    def zpass(zz, i, rel, r0=0, rn=128):
        ref = wrows(zz, i, r0, rn)
        post.send(("zp", rel, i, r0), ref, ref, partner)

    def ocols(zz, core=c, r0=0, rn=256):
        return wo.at[pl.ds(r0, rn), cols_at((zz * 4 + 2 * core) * 128, 256)]

    def osend(zz, r, d, r0=0, rn=256):
        ref = ocols(zz, c, r0, rn)
        post.send(("o", d, r), ref, ref, at(x, y, zp if d == "m" else zm, c))

    def opass(zz, rel, r0=0, rn=256):
        ref = ocols(zz, c, r0, rn)
        post.send(("op", rel, r0), ref, ref, partner)

    for i in (0, 1):
        post.recv("w", wrows(z, i), None, rs.at[post.ids["w0"] + (yl if i == 0 else 1 - yl)])
        for d in ("m", "p"):
            zsend(z, i, 1, d)
        zpass(z, i, 0)
    post.send("dec", decp, dec, partner, own)

    cm, cp, c2 = ym // 2 == c, yp // 2 == c, y2 // 2 == c
    post.recv("x1m", xblock(y, 0, 0, 128, xm * 1024, 1024), own)
    ref = xblock(y, 0, 0, 64, xm * 1024, 1024)
    post.send("x1m2", ref, ref, at(xp, y, z, c), own)
    post.recv("x1p", xblock(y, 0, 0, 128, xp * 1024, 1024), own)
    ref = xblock(y, 0, 64, 64, xp * 1024, 1024)
    post.send("x1p2", ref, ref, at(xm, y, z, c), own)
    post.recv("x2m", xblock(ym, 1, 0, 128, x * 1024, 1024), cm)
    ref = xblock(ym, 1, 0, 64, x * 1024, 1024)
    post.send("x2m2", ref, ref, at(x, yp, z, c), cm)
    post.recv("x2p", xblock(yp, 1, 0, 128, x * 1024, 1024), cp)
    ref = xblock(yp, 1, 64, 64, x * 1024, 1024)
    post.send("x2p2", ref, ref, at(x, ym, z, c), cp)

    for name, half in (("x1", 0), ("x2", 1)):
        block = xblock(y, half, 0, 128, mine, 512)
        post.recv(name + "s", block, own)
        post.recv(name + "l", xblock(y, half, 0, 128, (x * 2 + 1 - c) * 512, 512), own)
    post.recv("x1m2", xblock(y, 0, 0, 64, x2 * 1024, 1024), own)
    post.recv("x1p2", xblock(y, 0, 64, 64, x2 * 1024, 1024), own)
    for i in (0, 1):
        ref = xblock(y, 0, i * 64, 64, 0, 4096)
        post.send(("x3m", i), ref, ref, at(x, yp, z, c), own)
    for i in (1, 0):
        ref = xblock(y, 0, i * 64, 64, 0, 4096)
        post.send(("x3p", i), ref, ref, at(x, ym, z, c), own)
    post.recv("x2m2", xblock(y2, 1, 0, 64, x * 1024, 1024), c2)
    post.recv("x2p2", xblock(y2, 1, 64, 64, x * 1024, 1024), c2)

    def x4(qx, k):
        return xblock(k, 1, 0, 128, qx * 1024, 1024)

    for d, to, order in (("m", xp, (0, 1)), ("p", xm, (1, 0))):
        for k in order:
            post.send(("x4" + d, k), x4(x, k), x4(x, k), at(to, y, z, c))

    def zstep(r):
        for i in (0, 1):
            for d in ("m", "p"):
                zz = (z - r) % 8 if d == "m" else (z + r) % 8
                post.recv(("z", d, r, i), wrows(zz, i))
                if r < 3:
                    zsend(zz, i, r + 1, d)
                else:
                    zsend(zz, i, 4, d, 0 if d == "m" else 64, 64)
                zpass(zz, i, -r % 8 if d == "m" else r)

    def ostep(r):
        for d in ("m", "p"):
            zz = (z - r) % 8 if d == "m" else (z + r) % 8
            post.recv(("o", d, r), ocols(zz))
            if r < 3:
                osend(zz, r + 1, d)
            else:
                osend(zz, 4, d, 0 if d == "m" else 128, 128)
            opass(zz, -r % 8 if d == "m" else r)

    zstep(1)
    post.recv(("x3m", 0), xblock(ym, 0, 0, 64, 0, 4096), cm)
    ref = xblock(ym, 0, 0, 64, 0, 4096)
    post.send("x3m2", ref, ref, at(x, yp, z, c), cm)
    post.recv(("x3p", 1), xblock(yp, 0, 64, 64, 0, 4096), cp)
    ref = xblock(yp, 0, 64, 64, 0, 4096)
    post.send("x3p2", ref, ref, at(x, ym, z, c), cp)
    post.recv(("x4m", 0), x4(xm, 0))
    post.send("x4m2", x4(xm, 0), x4(xm, 0), at(xp, y, z, c))
    post.recv(("x4p", 1), x4(xp, 1))
    post.send("x4p2", x4(xp, 1), x4(xp, 1), at(xm, y, z, c))
    zstep(2)
    post.recv("o", ocols(z))
    zstep(3)
    for d in ("m", "p"):
        osend(z, 1, d)
    opass(z, 0)
    post.recv(("x3m", 1), xblock(ym, 0, 64, 64, 0, 4096), cm)
    post.recv(("x3p", 0), xblock(yp, 0, 0, 64, 0, 4096), cp)
    post.recv("x3m2", xblock(y2, 0, 0, 64, 0, 4096), c2)
    post.recv("x3p2", xblock(y2, 0, 64, 64, 0, 4096), c2)
    post.recv(("x4m", 1), x4(xm, 1))
    post.recv(("x4p", 0), x4(xp, 0))
    post.recv("x4m2", x4(x2, 0))
    post.recv("x4p2", x4(x2, 1))
    for name, ref in (("gain", gain), ("cos", cosine), ("sin", sine), ("base", base), ("dk", dk), ("pv", pv)):
        post.recv(name, ref)

    @pl.loop(0, ROWS // 128)
    def _(i):
        rows = rows_at(i * 128, 128)
        square = jnp.zeros((128, 128), F32)
        for k in range(32):
            piece = xg[rows, k * 128 : k * 128 + 128].astype(F32)
            square = square + piece * piece
        scale = lax.rsqrt(jnp.sum(square, axis=1, keepdims=True) / 4096 + EPS)
        for k in range(32):
            cols = slice(k * 128, k * 128 + 128)
            nrm[rows, cols] = (xg[rows, cols].astype(F32) * scale * gain[:, cols]).astype(BF)

    far = (z + 4) % 8
    for i in (0, 1):
        for d, r0 in (("m", 0), ("p", 64)):
            post.recv(("z", d, 4, i), wrows(far, i, r0, 64))
            zpass(far, i, 4, r0, 64)
    ostep(1)
    post.recv("dec", dec, other)

    @pl.when(own)
    def _():
        dec[...] = decp[...]

    for rel in range(8):
        zz = (z + rel) % 8
        for i in (0, 1):
            sub = yl if i == 0 else 1 - yl
            for r0, rn in ((0, 64), (64, 64)) if rel == 4 else ((0, 128),):
                row = (zz * 4 + 2 * (1 - c) + sub) * 128 + r0
                post.recv(("zp", rel, i, r0), wt.at[rows_at(row, rn), :])

    proj = dot(nrm[...], wt[...]).astype(BF)
    cb, sb = base[n][:, 0:128], base[n][:, 128:256]
    cosine[...], sine[...] = cosine[...] * cb - sine[...] * sb, sine[...] * cb + cosine[...] * sb

    def turn(rows):
        wide = rows.astype(F32)
        return (wide * cosine[...] + pltpu.roll(wide, 64, axis=1) * sine[...]).astype(BF)

    keys, values = turn(proj[:, 128:256]), proj[:, 256:384]
    us[...] = (proj[:, 512:640].astype(F32) * jax.nn.sigmoid(proj[:, 640:768].astype(F32))).astype(BF)
    after, before = (n + 1) % 16, (n + 15) % 16
    post.send("ht", us.at[pl.ds(ROWS - 16, 16), :], halo.at[0], at(x, y, after // 2, after % 2))
    post.send("hh", us.at[pl.ds(0, 16), :], halo.at[1], at(x, y, before // 2, before % 2))
    lf, lb = dec[0:1, :], dec[1:2, :]
    place_ = lax.broadcasted_iota(jnp.int32, (ROWS, 128), 0).astype(F32)
    wide = keys.astype(F32)
    st[0] = dot((wide * jnp.exp(lb * place_)).astype(BF), values, ((0,), (0,))).astype(BF)
    st[1] = dot((wide * jnp.exp(lf * (ROWS - 1.0 - place_))).astype(BF), values, ((0,), (0,))).astype(BF)
    for dz, q in line:
        post.send(("st", dz), st.at[(q * 2 - z * 2 + 16) // 16], sg.at[n], at(x, y, q, c))
    post.send("sp", st.at[1 - c], sg.at[n], partner)
    queries = turn(proj[:, 0:128])
    gs[...] = proj[:, 384:512]
    qs[...] = queries
    f1, b1 = lf[:, 0:1], lb[:, 0:1]
    for i in range(ROWS // 128):
        rows = slice(i * 128, i * 128 + 128)
        gap = (
            lax.broadcasted_iota(jnp.int32, (128, ROWS), 0)
            + i * 128
            - lax.broadcasted_iota(jnp.int32, (128, ROWS), 1)
        ).astype(F32)
        decay = jnp.exp(jnp.where(gap >= 0, f1 * gap, -b1 * gap))
        scores = dot(queries[rows], keys, ((1,), (1,))) * decay
        inner[rows, :] = dot(scores.astype(BF), values)
    ostep(2)

    post.recv("ht", halo.at[0])
    post.recv("hh", halo.at[1])
    pad[0:16, :] = jnp.where(n > 0, halo[0].astype(F32), 0.0)
    pad[16 : 16 + ROWS, :] = us[...].astype(F32)
    pad[16 + ROWS :, :] = jnp.where(n < 15, halo[1].astype(F32), 0.0)
    lane = lax.broadcasted_iota(jnp.int32, (128, 128), 1)
    for i in range(ROWS // 128):
        filtered = jnp.broadcast_to(pv[0:1, :], (128, 128))
        for t in range(KERNEL):
            filtered = filtered + dk[t : t + 1, :] * pad[i * 128 + t + 1 : i * 128 + t + 129, :]
        filt[i * 128 : i * 128 + 128, :] = filtered
        total = jnp.sum(filtered, axis=1, keepdims=True)
        square = jnp.sum(filtered * filtered, axis=1, keepdims=True)
        tile = jnp.where(lane == 0, total, jnp.where(lane == 1, square, 0.0))
        stat[:, i * 128 : i * 128 + 128] = tile.T[0:8, :]
    me = x * 4 + y
    for i in range(4):
        for j in range(4):
            if i or j:
                post.send("stats", stat, stats.at[me], at((x + i) % 4, (y + j) % 4, z, c))
    stats[pl.ds(me, 1)] = stat[...][None]
    sg[pl.ds(n, 1)] = jnp.zeros((1, 128, 128), BF)

    for dz, q in line:
        slot = sg.at[((z - dz) % 8) * 2 + c]
        post.recv(("st", dz), slot)
        post.send(("sp", dz), slot, slot, partner)
    ostep(3)
    post.recv("sp", sg.at[z * 2 + 1 - c])
    for dz, q in line:
        post.recv(("sp", dz), sg.at[((z - dz) % 8) * 2 + 1 - c])
    enter_f, enter_b = jnp.zeros((128, 128), F32), jnp.zeros((128, 128), F32)
    for j in range(16):
        state = sg[j].astype(F32)
        ahead, behind = n - 1 - j, j - n - 1
        wf = jnp.exp(lf * (ROWS * jnp.maximum(ahead, 0)).astype(F32))
        wb_ = jnp.exp(lb * (ROWS * jnp.maximum(behind, 0)).astype(F32))
        enter_f = enter_f + jnp.where(ahead >= 0, wf, 0.0) * state
        enter_b = enter_b + jnp.where(behind >= 0, wb_, 0.0) * state
    wide = qs[...].astype(F32)
    retained = inner[...]
    retained = retained + dot((wide * jnp.exp(lf * (place_ + 1.0))).astype(BF), enter_f.astype(BF))
    retained = retained + dot((wide * jnp.exp(lb * (ROWS - place_))).astype(BF), enter_b.astype(BF))
    mean = jnp.mean(retained, axis=-1, keepdims=True)
    centered = retained - mean
    variance = jnp.mean(centered * centered, axis=-1, keepdims=True)
    scaled = centered * lax.rsqrt(variance + EPS) * pv[3:4, :] + pv[4:5, :]
    both[:, 0:128] = (jax.nn.silu(gs[...].astype(F32)) * scaled).astype(BF)

    for d, r0 in (("m", 0), ("p", 128)):
        post.recv(("o", d, 4), ocols(far, c, r0, 128))
        opass(far, 4, r0, 128)
    post.recv("stats", stats.at[pl.ds(0, 15)])
    total = stats[0]
    for j in range(1, 16):
        total = total + stats[j]
    for i in range(ROWS // 128):
        rows = slice(i * 128, i * 128 + 128)
        tall = jnp.concatenate([total[:, rows], jnp.zeros((120, 128), F32)], axis=0).T
        mean = tall[:, 0:1] / CONV_WIDTH
        variance = tall[:, 1:2] / CONV_WIDTH - mean * mean
        leveled = (filt[rows, :] - mean) * lax.rsqrt(variance + EPS) * pv[1:2, :] + pv[2:3, :]
        both[rows, 128:256] = jax.nn.silu(leveled).astype(BF)
    for rel in range(8):
        zz = (z + rel) % 8
        for r0, rn in ((0, 128), (128, 128)) if rel == 4 else ((0, 256),):
            post.recv(("op", rel, r0), ocols(zz, 1 - c, r0, rn))

    def out_part(first, last):
        for k in range(first, last):
            cols = slice(k * 512, k * 512 + 512)
            part[:, :, :, :, cols] = dot(both[...], wo[:, cols]).astype(BF).reshape(2, 4, 2, 32, 512)

    left, right = pl.ds(0, 2048), pl.ds(2048, 2048)
    to_xp, to_xm = at(xp, y, z, c), at(xm, y, z, c)
    c1p, c1m = cp, cm

    def pa(k, q):
        return part.at[k, q, :, :, left]

    def pb(yy, q0, k):
        return part.at[yy % 2, pl.ds(q0, 2), k, :, right]

    out_part(0, 4)
    post.send("a2m", pa(0, x2), a2m, to_xp)
    post.send("a2p", pa(1, x2), a2p, to_xm)
    post.send("am1", pa(1, xp), am.at[1], to_xp)
    post.send("ap0", pa(0, xm), ap.at[0], to_xm)
    out_part(4, 8)
    for k in (0, 1):
        post.send("b2m", pb(y2, 0, k), b2m.at[k], at(x, yp, z, c), c2)
        post.send("b2p", pb(y2, 2, k), b2p.at[k], at(x, ym, z, c), c2)
    for k in (0, 1):
        post.send("bm1", pb(yp, 2, k), bm.at[pl.ds(2, 2)], at(x, yp, z, k), c1p)
        post.send("bp0", pb(ym, 0, k), bp.at[pl.ds(0, 2)], at(x, ym, z, k), c1m)
    post.send("bo", part.at[y % 2, :, 1 - c, :, right], bo, partner, own)

    def add(a, b):
        return (a.astype(F32) + b.astype(F32)).astype(BF)

    post.recv("a2m", a2m)
    ta[0] = add(a2m[...], part[0, xp, :, :, 0:2048])
    post.send("am0", ta.at[0], am.at[0], to_xp)
    post.recv("a2p", a2p)
    ta[1] = add(a2p[...], part[1, xm, :, :, 0:2048])
    post.send("ap1", ta.at[1], ap.at[1], to_xm)

    post.recv("b2m", b2m, c1p)

    @pl.when(c1p)
    def _():
        for k in (0, 1):
            tb[0, k] = add(b2m[k], part[yp % 2, 0:2, k, :, 2048:4096])

    for k in (0, 1):
        post.send("bm0", tb.at[0, k], bm.at[pl.ds(0, 2)], at(x, yp, z, k), c1p)
    post.recv("b2p", b2p, c1m)

    @pl.when(c1m)
    def _():
        for k in (0, 1):
            tb[1, k] = add(b2p[k], part[ym % 2, 2:4, k, :, 2048:4096])

    for k in (0, 1):
        post.send("bp1", tb.at[1, k], bp.at[pl.ds(2, 2)], at(x, ym, z, k), c1m)

    @pl.when(own)
    def _():
        bo[...] = part[y % 2, :, c, :, 2048:4096]

    post.recv("am1", am.at[1])
    post.recv("ap0", ap.at[0])
    post.recv("am0", am.at[0])
    post.recv("ap1", ap.at[1])
    for k in (0, 1):
        u[k] = (part[k, x, :, :, 0:2048].astype(F32) + am[k].astype(F32) + ap[k].astype(F32)).astype(BF)
    for k in (0, 1):
        for k2 in (0, 1):
            q = 2 * c + k
            here = (q == y) & (k2 == c)
            post.send("ua", u.at[k, k2], ua.at[y], at(x, q, z, k2), jnp.logical_not(here))
            post.local("ua", u.at[k, k2], ua.at[y], here)
    post.recv("bm1", bm.at[pl.ds(2, 2)])
    post.recv("bp0", bp.at[pl.ds(0, 2)])
    post.recv("bo", bo, other)
    post.recv("bm0", bm.at[pl.ds(0, 2)])
    post.recv("bp1", bp.at[pl.ds(2, 2)])
    for q in range(4):
        v[q] = (bm[q].astype(F32) + bp[q].astype(F32) + bo[q].astype(F32)).astype(BF)
    for d, q in (("2", x2), ("p", xp), ("m", xm)):
        post.send("vb", v.at[q], vb.at[x], at(q, y, z, c))
    post.recv("ua", ua)
    out[:, 0:2048] = (
        ua[0].astype(F32) + ua[1].astype(F32) + ua[2].astype(F32) + ua[3].astype(F32)
    ).astype(BF)
    vb[pl.ds(x, 1)] = v[pl.ds(x, 1)]
    post.recv("vb", vb.at[pl.ds(0, 3)])
    out[:, 2048:4096] = (
        vb[0].astype(F32) + vb[1].astype(F32) + vb[2].astype(F32) + vb[3].astype(F32)
    ).astype(BF)
    post.finish()


def table():
    half = HEAD_DIM // 2
    inverse = np.tile(THETA ** (-np.arange(half) / half), 2)
    sign = np.repeat([-1.0, 1.0], half)
    near = np.arange(ROWS)[:, None] * inverse
    far = np.arange(16)[:, None] * ROWS * inverse
    base = np.concatenate([np.cos(far), sign * np.sin(far)], axis=1)
    return [a.astype(np.float32) for a in (np.cos(near), sign * np.sin(near), base[:, None])]


def shards(
    hidden_states,
    norm_gain,
    query_weight,
    key_weight,
    value_weight,
    output_gate_weight,
    unit_input_weight,
    unit_gate_weight,
    decay_forward,
    decay_backward,
    group_gain,
    group_bias,
    depth_kernel,
    depth_bias,
    channel_gain,
    channel_bias,
    retention_out_weight,
    convolution_out_weight,
):
    vectors = jnp.stack([depth_bias, channel_gain, channel_bias, group_gain, group_bias])
    buf = lambda *shape: pltpu.VMEM((*shape, 2048), BF)
    small = lambda dtype: pltpu.VMEM((ROWS, 128), dtype)
    return pl.pallas_call(
        mixer_kernel,
        name="mixer",
        out_shape=jax.ShapeDtypeStruct((32, 4096), BF),
        in_specs=[HBM] * 15 + [SM] * 2,
        out_specs=VM,
        scratch_shapes=[
            pltpu.VMEM((ROWS, 4096), BF),
            pltpu.VMEM((ROWS, 4096), BF),
            pltpu.VMEM((4096, 768), BF),
            pltpu.VMEM((256, 4096), BF),
            pltpu.VMEM((KERNEL, 128), F32),
            pltpu.VMEM((5, 128), F32),
            pltpu.VMEM((1, 4096), F32),
            small(F32),
            small(F32),
            pltpu.VMEM((16, 1, 256), F32),
            pltpu.VMEM((8, 128), F32),
            pltpu.VMEM((8, 128), F32),
            small(BF),
            small(F32),
            small(BF),
            small(BF),
            pltpu.VMEM((2, 128, 128), BF),
            pltpu.VMEM((16, 128, 128), BF),
            pltpu.VMEM((2, 16, 128), BF),
            pltpu.VMEM((ROWS + 32, 128), F32),
            small(F32),
            pltpu.VMEM((8, ROWS), F32),
            pltpu.VMEM((16, 8, ROWS), F32),
            pltpu.VMEM((ROWS, 256), BF),
            pltpu.VMEM((2, 4, 2, 32, 4096), BF),
            buf(2, 32),
            buf(2, 32),
            buf(2, 2, 32),
            buf(2, 2, 32),
            buf(2, 2, 32),
            buf(2, 2, 32),
            buf(4, 32),
            buf(2, 2, 32),
            buf(2, 2, 32),
            buf(4, 32),
            buf(4, 32),
            buf(4, 32),
            buf(2, 2, 2, 32),
            buf(4, 32),
            buf(4, 32),
            pltpu.SemaphoreType.DMA((200,)),
            pltpu.SemaphoreType.DMA((140,)),
        ],
        compiler_params=pltpu.CompilerParams(
            collective_id=0, has_side_effects=True, vmem_limit_bytes=48 * MIB
        ),
    )(
        hidden_states,
        query_weight,
        key_weight,
        value_weight,
        output_gate_weight,
        unit_input_weight,
        unit_gate_weight,
        retention_out_weight,
        convolution_out_weight,
        depth_kernel,
        vectors,
        norm_gain.reshape(1, -1),
        *table(),
        decay_forward,
        decay_backward,
    )


def solution(mesh):
    split = P("sp", "tp")
    placed = (
        (split, P())
        + (split,) * 6
        + (P("tp"),) * 4
        + (P(None, "tp"),)
        + (P("tp"),) * 3
        + (P("tp", "sp"),) * 2
    )
    return jax.shard_map(
        shards, mesh=mesh, in_specs=placed, out_specs=P(("sp", "tp"), None), check_vma=False
    )
```

```python
import functools

import jax
import jax.numpy as jnp
import numpy as np
from jax import lax
from jax.experimental import pallas as pl
from jax.experimental.pallas import tpu as pltpu
from jax.sharding import PartitionSpec as P

HEAD_DIM = 128
CONV_WIDTH = 2048
KERNEL = 31
EPS = 1e-06
THETA = 10000.0
ROWS = 512
ORDER = (0, 1, 7, 2, 6, 3, 5, 4)
BF = jnp.bfloat16
F32 = jnp.float32
MESH = pl.DeviceIdType.MESH
VM = pl.BlockSpec(memory_space=pltpu.VMEM)
HBM = pl.BlockSpec(memory_space=pltpu.HBM)
SM = pl.BlockSpec(memory_space=pltpu.SMEM)
MIB = 1 << 20


def place():
    sp, tp = lax.axis_index("sp"), lax.axis_index("tp")
    return tp // 2, sp % 4, sp // 4, tp % 2


def at(x, y, z, c):
    return (z * 4 + y, x * 2 + c)


def when(cond, f):
    if cond is None:
        f()
    else:
        pl.when(cond)(f)


class Post:
    def __init__(self, send_sems, recv_sems):
        self.ss, self.rs = send_sems, recv_sems
        self.sent, self.ids = [], {}

    def key(self, name):
        return self.rs.at[self.ids.setdefault(name, len(self.ids))]

    def send(self, name, src, dst, to, cond=None, recv=None):
        sem = self.ss.at[len(self.sent)]
        recv = self.key(name) if recv is None else recv

        def make():
            return pltpu.make_async_remote_copy(
                src_ref=src, dst_ref=dst, send_sem=sem, recv_sem=recv, device_id=to, device_id_type=MESH
            )

        self.sent.append((make, cond))
        when(cond, lambda: make().start())

    def local(self, name, src, dst, cond=None, recv=None):
        recv = self.key(name) if recv is None else recv
        when(cond, lambda: pltpu.make_async_copy(src, dst, recv).start())

    def recv(self, name, ref, cond=None, recv=None):
        recv = self.key(name) if recv is None else recv
        when(cond, lambda: pltpu.make_async_copy(ref, ref, recv).wait())

    def finish(self):
        for make, cond in self.sent:
            when(cond, lambda: make().wait_send())


def greet(peers):
    barrier = pltpu.get_barrier_semaphore()
    for peer in peers:
        pl.semaphore_signal(barrier, inc=1, device_id=peer, device_id_type=MESH)
    pl.semaphore_wait(barrier, len(peers))


def rows_at(start, size, unit=16):
    return pl.ds(pl.multiple_of(start, unit), size)


def cols_at(start, size):
    return pl.ds(pl.multiple_of(start, 128), size)


def dot(a, b, dims=((1,), (0,))):
    return lax.dot_general(a, b, (dims, ((), ())), preferred_element_type=F32)


def log_sigmoid(decay):
    t = jnp.exp(-decay)
    s = t / (2.0 + t)
    square = s * s
    series = jnp.full_like(s, 1.0 / 15)
    for n in (13, 11, 9, 7, 5, 3, 1):
        series = series * square + 1.0 / n
    return -2.0 * s * series


def mixer_kernel(
    xin, wq, wk, wv, wg, wa, wb, wr, wc, dk_in, v0, v1, v2, v3, v4, gain_in, cos_in, sin_in, base_in, df, db, out,
    xg, nrm, wt, wo, dk, pv, gain, cosine, sine, base, dec, decp, qs, inner, gs, us, st, sp, chip, sg, halo,
    pad, filt, stat, stats, both, part, acc,
    a2m, a2p, am, ap, ta, u, ua, b2m, b2p, bm, bp, bo, tb, v, vb, ss, rs,
):
    pv_in = (v0, v1, v2, v3, v4)
    x, y, z, c = place()
    n = z * 2 + c
    ct, yl = y // 2, y % 2
    xp, xm, x2 = (x + 1) % 4, (x + 3) % 4, (x + 2) % 4
    yp, ym, y2 = (y + 1) % 4, (y + 3) % 4, (y + 2) % 4
    zp, zm = (z + 1) % 8, (z + 7) % 8
    own = ct == c
    other = ct != c
    post = Post(ss, rs)
    partner = at(x, y, z, 1 - c)
    post.local("gain", gain_in, gain)
    post.local("cos", cos_in, cosine)
    post.local("sin", sin_in, sine)
    post.local("base", base_in, base)
    line = [(dz, (z + dz) % 8) for dz in range(1, 8)]
    greet(
        [at(q, y, z, k) for q in (xp, xm) for k in (0, 1)]
        + [at(x, q, z, k) for q in (yp, ym, y2) for k in (0, 1)]
        + [at(x, y, zp, c), at(x, y, zm, c), partner]
    )

    def xblock(yy, half, r0, rn, col, width):
        return xg.at[rows_at((yy % 2) * 256 + half * 128 + r0, rn), cols_at(col, width)]

    s = z * 4 + y
    post.key("w0"), post.key("w1")
    wsem = rs.at[post.ids["w0"] + yl]

    def wstart(near):
        j = 1 - yl if near else yl
        to = at(x, 2 * c + j, z, ct)
        for m, w in enumerate((wq, wk, wv, wg, wa, wb)):
            src, dst = w.at[:, cols_at(j * 128, 128)], wt.at[rows_at(s * 128, 128), pl.ds(m * 128, 128)]
            if near:
                post.send("w", src, dst, to, None, wsem)
            else:
                post.local("w", src, dst, own, wsem)
                post.send("w", src, dst, to, other, wsem)

    def ostart(near):
        j = 1 - yl if near else yl
        to = at(x, 2 * c + j, z, ct)
        for m, w in enumerate((wr, wc)):
            src, dst = w.at[rows_at(j * 128, 128), :], wo.at[pl.ds(m * 128, 128), cols_at(s * 128, 128)]
            if near:
                post.send("o", src, dst, to)
            else:
                post.local("o", src, dst, own)
                post.send("o", src, dst, to, other)

    wstart(True)
    mine = (x * 2 + c) * 512
    for half, name, ends in ((1, "x2", ((x, yp, "m"), (x, ym, "p"))), (0, "x1", ((xp, y, "m"), (xm, y, "p")))):
        src, dst = xin.at[pl.ds(half * 128, 128), :], xblock(y, half, 0, 128, mine, 512)
        for qx, qy, d in ends:
            post.send(name + d, src, dst, at(qx, qy, z, ct))
        post.send(name + "l", src, dst, partner, other)
        post.local(name + "s", src, dst, own)
    wstart(False)
    for name, ref, dst in (("dk", dk_in, dk), *((("v", i), r, pv.at[i]) for i, r in enumerate(pv_in))):
        src = ref.at[:, cols_at(yl * 128, 128)]
        post.send(name, src, dst, partner, own)
        post.local(name, src, dst, own)
    decp[0:1, :] = log_sigmoid(jnp.full((1, 128), df[yl], F32))
    decp[1:2, :] = log_sigmoid(jnp.full((1, 128), db[yl], F32))

    first = (yl + c + ct) % 2

    def wrows(zz, i, r0=0, rn=128):
        sub = first if i == 0 else 1 - first
        return wt.at[rows_at((zz * 4 + 2 * c + sub) * 128 + r0, rn), :]

    def zsend(zz, i, r, d, r0=0, rn=128):
        ref = wrows(zz, i, r0, rn)
        post.send(("z", d, r, i), ref, ref, at(x, y, zp if d == "m" else zm, c))

    def zpass(zz, i, rel, r0=0, rn=128):
        ref = wrows(zz, i, r0, rn)
        post.send(("zp", rel, i, r0), ref, ref, partner)

    def ocols(zz, i, core=c):
        return wo.at[:, cols_at((zz * 4 + 2 * core + i) * 128, 128)]

    def osend(zz, i, r, d):
        post.send(("o", d, r, i), ocols(zz, i), ocols(zz, i), at(x, y, zp if d == "m" else zm, c))

    def opass(zz, i, rel):
        post.send(("op", rel, i), ocols(zz, i), ocols(zz, i), partner)

    def wfirst(i):
        post.recv("w", wrows(z, i), None, rs.at[post.ids["w0"] + (first if i == 0 else 1 - first)])
        for d in ("m", "p"):
            zsend(z, i, 1, d)
        zpass(z, i, 0)

    wfirst(0)
    cm, cp, c2 = ym // 2 == c, yp // 2 == c, y2 // 2 == c
    post.recv("x1m", xblock(y, 0, 0, 128, xm * 1024, 1024), own)
    ref = xblock(y, 0, 0, 64, xm * 1024, 1024)
    post.send("x1m2", ref, ref, at(xp, y, z, c), own)
    post.recv("x1p", xblock(y, 0, 0, 128, xp * 1024, 1024), own)
    ref = xblock(y, 0, 64, 64, xp * 1024, 1024)
    post.send("x1p2", ref, ref, at(xm, y, z, c), own)
    post.recv("x2m", xblock(ym, 1, 0, 128, x * 1024, 1024), cm)
    ref = xblock(ym, 1, 0, 64, x * 1024, 1024)
    post.send("x2m2", ref, ref, at(x, yp, z, c), cm)
    post.recv("x2p", xblock(yp, 1, 0, 128, x * 1024, 1024), cp)
    ref = xblock(yp, 1, 64, 64, x * 1024, 1024)
    post.send("x2p2", ref, ref, at(x, ym, z, c), cp)

    for name, half in (("x1", 0), ("x2", 1)):
        post.recv(name + "s", xblock(y, half, 0, 128, mine, 512), own)
        post.recv(name + "l", xblock(y, half, 0, 128, (x * 2 + 1 - c) * 512, 512), own)
    post.recv("x1m2", xblock(y, 0, 0, 64, x2 * 1024, 1024), own)
    post.recv("x1p2", xblock(y, 0, 64, 64, x2 * 1024, 1024), own)
    for i in (0, 1):
        ref = xblock(y, 0, i * 64, 64, 0, 4096)
        post.send(("x3m", i), ref, ref, at(x, yp, z, c), own)
    for i in (1, 0):
        ref = xblock(y, 0, i * 64, 64, 0, 4096)
        post.send(("x3p", i), ref, ref, at(x, ym, z, c), own)
    wfirst(1)
    post.recv("x2m2", xblock(y2, 1, 0, 64, x * 1024, 1024), c2)
    post.recv("x2p2", xblock(y2, 1, 64, 64, x * 1024, 1024), c2)

    def x4(qx, k):
        return xblock(k, 1, 0, 128, qx * 1024, 1024)

    for d, to, order in (("m", xp, (0, 1)), ("p", xm, (1, 0))):
        for k in order:
            post.send(("x4" + d, k), x4(x, k), x4(x, k), at(to, y, z, c))
    ostart(True)
    ostart(False)
    post.send("dec", decp, dec, partner, own)

    def zstep(r, parts=(0, 1)):
        for i in parts:
            for d in ("m", "p"):
                zz = (z - r) % 8 if d == "m" else (z + r) % 8
                post.recv(("z", d, r, i), wrows(zz, i))
                if r < 3:
                    zsend(zz, i, r + 1, d)
                else:
                    zsend(zz, i, 4, d, 0 if d == "m" else 64, 64)
                zpass(zz, i, -r % 8 if d == "m" else r)

    def ostep(r, i):
        for d in ("m", "p"):
            zz = (z - r) % 8 if d == "m" else (z + r) % 8
            if r == 4 and i != (d == "p"):
                continue
            post.recv(("o", d, r, i), ocols(zz, i))
            if r < 3 or (r == 3 and i == (d == "p")):
                osend(zz, i, r + 1, d)
            opass(zz, i, -r % 8 if d == "m" else r)

    zstep(1)
    post.recv(("x3m", 0), xblock(ym, 0, 0, 64, 0, 4096), cm)
    ref = xblock(ym, 0, 0, 64, 0, 4096)
    post.send("x3m2", ref, ref, at(x, yp, z, c), cm)
    post.recv(("x3p", 1), xblock(yp, 0, 64, 64, 0, 4096), cp)
    ref = xblock(yp, 0, 64, 64, 0, 4096)
    post.send("x3p2", ref, ref, at(x, ym, z, c), cp)
    post.recv(("x4m", 0), x4(xm, 0))
    post.send("x4m2", x4(xm, 0), x4(xm, 0), at(xp, y, z, c))
    post.recv(("x4p", 1), x4(xp, 1))
    post.send("x4p2", x4(xp, 1), x4(xp, 1), at(xm, y, z, c))
    zstep(2)
    post.recv("o", wo.at[:, cols_at((z * 4 + 2 * c) * 128, 256)])
    zstep(3, (0,))
    post.recv(("x3m", 1), xblock(ym, 0, 64, 64, 0, 4096), cm)
    post.recv(("x3p", 0), xblock(yp, 0, 0, 64, 0, 4096), cp)
    post.recv("x3m2", xblock(y2, 0, 0, 64, 0, 4096), c2)
    post.recv("x3p2", xblock(y2, 0, 64, 64, 0, 4096), c2)
    post.recv(("x4m", 1), x4(xm, 1))
    post.recv(("x4p", 0), x4(xp, 0))
    post.recv("x4m2", x4(x2, 0))
    post.recv("x4p2", x4(x2, 1))
    for name, ref in (("gain", gain), ("cos", cosine), ("sin", sine), ("base", base), ("dk", dk), *((("v", i), pv.at[i]) for i in range(5))):
        post.recv(name, ref)

    @pl.loop(0, ROWS // 128)
    def _(i):
        rows = rows_at(i * 128, 128)
        square = jnp.zeros((128, 128), F32)
        for k in range(32):
            piece = xg[rows, k * 128 : k * 128 + 128].astype(F32)
            square = square + piece * piece
        scale = lax.rsqrt(jnp.sum(square, axis=1, keepdims=True) / 4096 + EPS)
        for k in range(32):
            cols = slice(k * 128, k * 128 + 128)
            nrm[rows, cols] = (xg[rows, cols].astype(F32) * scale * gain[:, cols]).astype(BF)

    zstep(3, (1,))
    for i in (0, 1):
        for d in ("m", "p"):
            osend(z, i, 1, d)
    for i in (0, 1):
        opass(z, i, 0)

    def zpassed(rel):
        zz = (z + rel) % 8
        for i in (0, 1):
            sub = 1 - first if i == 0 else first
            for r0, rn in ((0, 64), (64, 64)) if rel == 4 else ((0, 128),):
                row = (zz * 4 + 2 * (1 - c) + sub) * 128 + r0
                post.recv(("zp", rel, i, r0), wt.at[rows_at(row, rn), :])

    def project(rel):
        start = ((z + rel) % 8) * 512
        return dot(nrm[:, cols_at(start, 512)], wt[rows_at(start, 512), :])

    far = (z + 4) % 8

    def projects(*rels):
        for rel in rels:
            zpassed(rel)
            acc[...] = project(rel) if rel == 0 else acc[...] + project(rel)

    projects(0, 1, 7, 2, 6)
    for i in (0, 1):
        for d, r0 in (("m", 0), ("p", 64)):
            post.recv(("z", d, 4, i), wrows(far, i, r0, 64))
            zpass(far, i, 4, r0, 64)
        projects(3 if i == 0 else 5)
    ostep(1, 0)
    post.recv("dec", dec, other)

    @pl.when(own)
    def _():
        dec[...] = decp[...]

    zpassed(4)
    proj = (acc[...] + project(4)).astype(BF)
    ostep(1, 1)
    cb, sb = base[n][:, 0:128], base[n][:, 128:256]
    cosine[...], sine[...] = cosine[...] * cb - sine[...] * sb, sine[...] * cb + cosine[...] * sb

    def turn(rows):
        wide = rows.astype(F32)
        return (wide * cosine[...] + pltpu.roll(wide, 64, axis=1) * sine[...]).astype(BF)

    keys, values = turn(proj[:, 128:256]), proj[:, 256:384]
    us[...] = (proj[:, 512:640].astype(F32) * jax.nn.sigmoid(proj[:, 640:768].astype(F32))).astype(BF)
    after, before = (n + 1) % 16, (n + 15) % 16
    post.send("ht", us.at[pl.ds(ROWS - 16, 16), :], halo.at[0], at(x, y, after // 2, after % 2))
    post.send("hh", us.at[pl.ds(0, 16), :], halo.at[1], at(x, y, before // 2, before % 2))
    lf, lb = dec[0:1, :], dec[1:2, :]
    place_ = lax.broadcasted_iota(jnp.int32, (ROWS, 128), 0).astype(F32)
    wide = keys.astype(F32)
    st[0] = dot((wide * jnp.exp(lb * place_)).astype(BF), values, ((0,), (0,))).astype(BF)
    st[1] = dot((wide * jnp.exp(lf * (ROWS - 1.0 - place_))).astype(BF), values, ((0,), (0,))).astype(BF)
    post.send("sp", st, sp, partner)
    queries = turn(proj[:, 0:128])
    gs[...] = proj[:, 384:512]
    qs[...] = queries
    f1, b1 = lf[:, 0:1], lb[:, 0:1]
    for i in range(ROWS // 128):
        rows = slice(i * 128, i * 128 + 128)
        gap = (
            lax.broadcasted_iota(jnp.int32, (128, ROWS), 0)
            + i * 128
            - lax.broadcasted_iota(jnp.int32, (128, ROWS), 1)
        ).astype(F32)
        decay = jnp.exp(jnp.where(gap >= 0, f1 * gap, -b1 * gap))
        scores = dot(queries[rows], keys, ((1,), (1,))) * decay
        inner[rows, :] = dot(scores.astype(BF), values)
    post.recv("sp", sp)
    span = jnp.exp(jnp.where(c == 1, lf, lb) * float(ROWS))
    chip[...] = (st[c].astype(F32) + span * sp[c].astype(F32)).astype(BF)

    def meant(a, b):
        return (a < b) == (c == 1)

    for dz, q in line:
        post.send(("st", dz), chip, sg.at[z], at(x, y, q, c), meant(z, q))
    ostep(2, 0)

    post.recv("ht", halo.at[0])
    post.recv("hh", halo.at[1])
    pad[0:16, :] = jnp.where(n > 0, halo[0].astype(F32), 0.0)
    pad[16 : 16 + ROWS, :] = us[...].astype(F32)
    pad[16 + ROWS :, :] = jnp.where(n < 15, halo[1].astype(F32), 0.0)
    lane = lax.broadcasted_iota(jnp.int32, (128, 128), 1)
    for i in range(ROWS // 128):
        filtered = jnp.broadcast_to(pv[0], (128, 128))
        for t in range(KERNEL):
            filtered = filtered + dk[t : t + 1, :] * pad[i * 128 + t + 1 : i * 128 + t + 129, :]
        filt[i * 128 : i * 128 + 128, :] = filtered
        total = jnp.sum(filtered, axis=1, keepdims=True)
        square = jnp.sum(filtered * filtered, axis=1, keepdims=True)
        tile = jnp.where(lane == 0, total, jnp.where(lane == 1, square, 0.0))
        stat[:, i * 128 : i * 128 + 128] = tile.T[0:8, :]
    ostep(2, 1)
    me = x * 4 + y
    for i in range(4):
        for j in range(4):
            if i or j:
                post.send("stats", stat, stats.at[me], at((x + i) % 4, (y + j) % 4, z, c))
    stats[pl.ds(me, 1)] = stat[...][None]
    for dz, q in line:
        source = (z - dz) % 8
        slot = sg.at[source]
        post.recv(("st", dz), slot, meant(source, z))
        post.send(("ss", dz), slot, slot, partner, meant(source, z))
    ostep(3, 0)
    sg[pl.ds(z, 1)] = jnp.zeros((1, 128, 128), BF)
    for dz, q in line:
        source = (z - dz) % 8
        post.recv(("ss", dz), sg.at[source], jnp.logical_not(meant(source, z)))
    enter_f, enter_b = jnp.zeros((128, 128), F32), jnp.zeros((128, 128), F32)
    for j in range(8):
        state = sg[j].astype(F32)
        ahead, behind = z - 1 - j, j - z - 1
        wf = jnp.exp(lf * (2 * ROWS * jnp.maximum(ahead, 0)).astype(F32))
        wb_ = jnp.exp(lb * (2 * ROWS * jnp.maximum(behind, 0)).astype(F32))
        enter_f = enter_f + jnp.where(ahead >= 0, wf, 0.0) * state
        enter_b = enter_b + jnp.where(behind >= 0, wb_, 0.0) * state
    enter_f = jnp.where(c == 1, jnp.exp(lf * float(ROWS)) * enter_f + sp[1].astype(F32), enter_f)
    enter_b = jnp.where(c == 0, jnp.exp(lb * float(ROWS)) * enter_b + sp[0].astype(F32), enter_b)
    wide = qs[...].astype(F32)
    retained = inner[...]
    retained = retained + dot((wide * jnp.exp(lf * (place_ + 1.0))).astype(BF), enter_f.astype(BF))
    retained = retained + dot((wide * jnp.exp(lb * (ROWS - place_))).astype(BF), enter_b.astype(BF))
    mean = jnp.mean(retained, axis=-1, keepdims=True)
    centered = retained - mean
    variance = jnp.mean(centered * centered, axis=-1, keepdims=True)
    scaled = centered * lax.rsqrt(variance + EPS) * pv[3] + pv[4]
    both[:, 0:128] = (jax.nn.silu(gs[...].astype(F32)) * scaled).astype(BF)

    ostep(3, 1)
    post.recv("stats", stats.at[pl.ds(0, 15)])
    total = stats[0]
    for j in range(1, 16):
        total = total + stats[j]
    for i in range(ROWS // 128):
        rows = slice(i * 128, i * 128 + 128)
        tall = jnp.concatenate([total[:, rows], jnp.zeros((120, 128), F32)], axis=0).T
        mean = tall[:, 0:1] / CONV_WIDTH
        variance = tall[:, 1:2] / CONV_WIDTH - mean * mean
        leveled = (filt[rows, :] - mean) * lax.rsqrt(variance + EPS) * pv[1] + pv[2]
        both[rows, 128:256] = jax.nn.silu(leveled).astype(BF)
    def out_part(slots):
        for k in slots:
            zz = (z + ORDER[k]) % 8
            for i in (0, 1):
                post.recv(("op", ORDER[k], i), ocols(zz, i, 1 - c))
            cols = slice(k * 512, k * 512 + 512)
            value = dot(both[...], wo[:, cols_at(zz * 512, 512)])
            part[:, :, :, :, cols] = value.astype(BF).reshape(2, 4, 2, 32, 512)

    to_xp, to_xm = at(xp, y, z, c), at(xm, y, z, c)
    c1p, c1m = cp, cm
    right = pl.ds(2560, 1536)
    groups = (pl.ds(0, 1536), pl.ds(1536, 1024))

    def add(a, b):
        return (a.astype(F32) + b.astype(F32)).astype(BF)

    def afirst(g):
        cols = groups[g]
        post.send(("a2m", g), part.at[0, x2, :, :, cols], a2m.at[:, :, cols], to_xp)
        post.send(("a2p", g), part.at[1, x2, :, :, cols], a2p.at[:, :, cols], to_xm)
        post.send(("am1", g), part.at[1, xp, :, :, cols], am.at[1, :, :, cols], to_xp)
        post.send(("ap0", g), part.at[0, xm, :, :, cols], ap.at[0, :, :, cols], to_xm)

    def asecond(g):
        cols = groups[g]
        post.recv(("a2m", g), a2m.at[:, :, cols])
        ta[0, :, :, cols] = add(a2m[:, :, cols], part[0, xp, :, :, cols])
        post.send(("am0", g), ta.at[0, :, :, cols], am.at[0, :, :, cols], to_xp)
        post.recv(("a2p", g), a2p.at[:, :, cols])
        ta[1, :, :, cols] = add(a2p[:, :, cols], part[1, xm, :, :, cols])
        post.send(("ap1", g), ta.at[1, :, :, cols], ap.at[1, :, :, cols], to_xm)

    def athird(g):
        cols = groups[g]
        for name, ref in (("am1", am.at[1]), ("ap0", ap.at[0]), ("am0", am.at[0]), ("ap1", ap.at[1])):
            post.recv((name, g), ref.at[:, :, cols])
        for k in (0, 1):
            value = part[k, x, :, :, cols].astype(F32) + am[k, :, :, cols].astype(F32)
            u[k, :, :, cols] = (value + ap[k, :, :, cols].astype(F32)).astype(BF)
        for k in (0, 1):
            for k2 in (0, 1):
                q = 2 * c + k
                here = (q == y) & (k2 == c)
                src, dst = u.at[k, k2, :, cols], ua.at[y, :, cols]
                post.send(("ua", g), src, dst, at(x, q, z, k2), jnp.logical_not(here))
                post.local(("ua", g), src, dst, here)

    def alast(g):
        cols = groups[g]
        post.recv(("ua", g), ua.at[:, :, cols])
        for k in range(cols.start // 512, (cols.start + cols.size) // 512):
            piece = slice(k * 512, k * 512 + 512)
            value = ua[0, :, piece].astype(F32)
            for q in (1, 2, 3):
                value = value + ua[q, :, piece].astype(F32)
            out[:, cols_at(((z + ORDER[k]) % 8) * 512, 512)] = value.astype(BF)

    def pb(yy, q0, k):
        return part.at[yy % 2, pl.ds(q0, 2), k, :, right]

    out_part((0, 1, 2))
    afirst(0)
    out_part((3, 4))
    afirst(1)
    for i in (0, 1):
        ostep(4, i)
    out_part((5, 6, 7))
    for k in (0, 1):
        post.send("b2m", pb(y2, 0, k), b2m.at[k], at(x, yp, z, c), c2)
        post.send("b2p", pb(y2, 2, k), b2p.at[k], at(x, ym, z, c), c2)
    for k in (0, 1):
        post.send("bm1", pb(yp, 2, k), bm.at[pl.ds(2, 2)], at(x, yp, z, k), c1p)
        post.send("bp0", pb(ym, 0, k), bp.at[pl.ds(0, 2)], at(x, ym, z, k), c1m)
    post.send("bo", part.at[y % 2, :, 1 - c, :, right], bo, partner, own)
    asecond(0)
    asecond(1)
    post.recv("b2m", b2m, c1p)

    @pl.when(c1p)
    def _():
        for k in (0, 1):
            tb[0, k] = add(b2m[k], part[yp % 2, 0:2, k, :, right])

    for k in (0, 1):
        post.send("bm0", tb.at[0, k], bm.at[pl.ds(0, 2)], at(x, yp, z, k), c1p)
    post.recv("b2p", b2p, c1m)

    @pl.when(c1m)
    def _():
        for k in (0, 1):
            tb[1, k] = add(b2p[k], part[ym % 2, 2:4, k, :, right])

    for k in (0, 1):
        post.send("bp1", tb.at[1, k], bp.at[pl.ds(2, 2)], at(x, ym, z, k), c1m)

    @pl.when(own)
    def _():
        bo[...] = part[y % 2, :, c, :, right]

    athird(0)
    post.recv("bm1", bm.at[pl.ds(2, 2)])
    post.recv("bp0", bp.at[pl.ds(0, 2)])
    post.recv("bo", bo, other)
    post.recv("bm0", bm.at[pl.ds(0, 2)])
    post.recv("bp1", bp.at[pl.ds(2, 2)])
    for q in range(4):
        v[q] = (bm[q].astype(F32) + bp[q].astype(F32) + bo[q].astype(F32)).astype(BF)
    for q in (x2, xp, xm):
        post.send("vb", v.at[q], vb.at[x], at(q, y, z, c))
    vb[pl.ds(x, 1)] = v[pl.ds(x, 1)]
    athird(1)
    alast(0)
    post.recv("vb", vb.at[pl.ds(0, 3)])
    for k in (5, 6, 7):
        piece = slice((k - 5) * 512, (k - 5) * 512 + 512)
        value = vb[0, :, piece].astype(F32)
        for q in (1, 2, 3):
            value = value + vb[q, :, piece].astype(F32)
        out[:, cols_at(((z + ORDER[k]) % 8) * 512, 512)] = value.astype(BF)
    alast(1)
    post.finish()


def table():
    half = HEAD_DIM // 2
    inverse = np.tile(THETA ** (-np.arange(half) / half), 2)
    sign = np.repeat([-1.0, 1.0], half)
    near = np.arange(ROWS)[:, None] * inverse
    far = np.arange(16)[:, None] * ROWS * inverse
    base = np.concatenate([np.cos(far), sign * np.sin(far)], axis=1)
    return [a.astype(np.float32) for a in (np.cos(near), sign * np.sin(near), base[:, None])]


def shards(
    hidden_states,
    norm_gain,
    query_weight,
    key_weight,
    value_weight,
    output_gate_weight,
    unit_input_weight,
    unit_gate_weight,
    decay_forward,
    decay_backward,
    group_gain,
    group_bias,
    depth_kernel,
    depth_bias,
    channel_gain,
    channel_bias,
    retention_out_weight,
    convolution_out_weight,
):
    vectors = (depth_bias, channel_gain, channel_bias, group_gain, group_bias)
    wide = lambda *shape: pltpu.VMEM((*shape, 2560), BF)
    narrow = lambda *shape: pltpu.VMEM((*shape, 1536), BF)
    small = lambda dtype: pltpu.VMEM((ROWS, 128), dtype)
    return pl.pallas_call(
        mixer_kernel,
        name="mixer",
        out_shape=jax.ShapeDtypeStruct((32, 4096), BF),
        in_specs=[HBM] * 19 + [SM] * 2,
        out_specs=VM,
        scratch_shapes=[
            pltpu.VMEM((ROWS, 4096), BF),
            pltpu.VMEM((ROWS, 4096), BF),
            pltpu.VMEM((4096, 768), BF),
            pltpu.VMEM((256, 4096), BF),
            pltpu.VMEM((KERNEL, 128), F32),
            pltpu.VMEM((5, 1, 128), F32),
            pltpu.VMEM((1, 4096), F32),
            small(F32),
            small(F32),
            pltpu.VMEM((16, 1, 256), F32),
            pltpu.VMEM((8, 128), F32),
            pltpu.VMEM((8, 128), F32),
            small(BF),
            small(F32),
            small(BF),
            small(BF),
            pltpu.VMEM((2, 128, 128), BF),
            pltpu.VMEM((2, 128, 128), BF),
            pltpu.VMEM((128, 128), BF),
            pltpu.VMEM((8, 128, 128), BF),
            pltpu.VMEM((2, 16, 128), BF),
            pltpu.VMEM((ROWS + 32, 128), F32),
            small(F32),
            pltpu.VMEM((8, ROWS), F32),
            pltpu.VMEM((16, 8, ROWS), F32),
            pltpu.VMEM((ROWS, 256), BF),
            pltpu.VMEM((2, 4, 2, 32, 4096), BF),
            pltpu.VMEM((ROWS, 768), F32),
            wide(2, 32),
            wide(2, 32),
            wide(2, 2, 32),
            wide(2, 2, 32),
            wide(2, 2, 32),
            wide(2, 2, 32),
            wide(4, 32),
            narrow(2, 2, 32),
            narrow(2, 2, 32),
            narrow(4, 32),
            narrow(4, 32),
            narrow(4, 32),
            narrow(2, 2, 2, 32),
            narrow(4, 32),
            narrow(4, 32),
            pltpu.SemaphoreType.DMA((230,)),
            pltpu.SemaphoreType.DMA((180,)),
        ],
        compiler_params=pltpu.CompilerParams(
            collective_id=0, has_side_effects=True, vmem_limit_bytes=67043328
        ),
    )(
        hidden_states,
        query_weight,
        key_weight,
        value_weight,
        output_gate_weight,
        unit_input_weight,
        unit_gate_weight,
        retention_out_weight,
        convolution_out_weight,
        depth_kernel,
        *(vector.reshape(1, -1) for vector in vectors),
        norm_gain.reshape(1, -1),
        *table(),
        decay_forward,
        decay_backward,
    )


def solution(mesh):
    split = P("sp", "tp")
    placed = (
        (split, P())
        + (split,) * 6
        + (P("tp"),) * 4
        + (P(None, "tp"),)
        + (P("tp"),) * 3
        + (P("tp", "sp"),) * 2
    )
    return jax.shard_map(
        shards, mesh=mesh, in_specs=placed, out_specs=P(("sp", "tp"), None), check_vma=False
    )
```

```python
import functools

import jax
import jax.numpy as jnp
import numpy as np
from jax import lax
from jax.experimental import pallas as pl
from jax.experimental.pallas import tpu as pltpu
from jax.sharding import PartitionSpec as P

HEAD_DIM = 128
CONV_WIDTH = 2048
KERNEL = 31
EPS = 1e-06
THETA = 10000.0
ROWS = 512
SPLIT = 96
ORDER = (0, 1, 7, 2, 6, 3, 5, 4)
BF = jnp.bfloat16
F32 = jnp.float32
MESH = pl.DeviceIdType.MESH
VM = pl.BlockSpec(memory_space=pltpu.VMEM)
HBM = pl.BlockSpec(memory_space=pltpu.HBM)
SM = pl.BlockSpec(memory_space=pltpu.SMEM)
MIB = 1 << 20


def place():
    sp, tp = lax.axis_index("sp"), lax.axis_index("tp")
    return tp // 2, sp % 4, sp // 4, tp % 2


def at(x, y, z, c):
    return (z * 4 + y, x * 2 + c)


def when(cond, f):
    if cond is None:
        f()
    else:
        pl.when(cond)(f)


class Post:
    def __init__(self, send_sems, recv_sems):
        self.ss, self.rs = send_sems, recv_sems
        self.sent, self.ids = [], {}

    def key(self, name):
        return self.rs.at[self.ids.setdefault(name, len(self.ids))]

    def send(self, name, src, dst, to, cond=None, recv=None):
        sem = self.ss.at[len(self.sent)]
        recv = self.key(name) if recv is None else recv

        def make():
            return pltpu.make_async_remote_copy(
                src_ref=src, dst_ref=dst, send_sem=sem, recv_sem=recv, device_id=to, device_id_type=MESH
            )

        self.sent.append((make, cond))
        when(cond, lambda: make().start())

    def local(self, name, src, dst, cond=None, recv=None):
        recv = self.key(name) if recv is None else recv
        when(cond, lambda: pltpu.make_async_copy(src, dst, recv).start())

    def recv(self, name, ref, cond=None, recv=None):
        recv = self.key(name) if recv is None else recv
        when(cond, lambda: pltpu.make_async_copy(ref, ref, recv).wait())

    def finish(self):
        for make, cond in self.sent:
            when(cond, lambda: make().wait_send())


def greet(peers):
    barrier = pltpu.get_barrier_semaphore()
    for peer in peers:
        pl.semaphore_signal(barrier, inc=1, device_id=peer, device_id_type=MESH)
    pl.semaphore_wait(barrier, len(peers))


def rows_at(start, size, unit=16):
    return pl.ds(pl.multiple_of(start, unit), size)


def cols_at(start, size):
    return pl.ds(pl.multiple_of(start, 128), size)


def dot(a, b, dims=((1,), (0,))):
    return lax.dot_general(a, b, (dims, ((), ())), preferred_element_type=F32)


def log_sigmoid(decay):
    t = jnp.exp(-decay)
    s = t / (2.0 + t)
    square = s * s
    series = jnp.full_like(s, 1.0 / 15)
    for n in (13, 11, 9, 7, 5, 3, 1):
        series = series * square + 1.0 / n
    return -2.0 * s * series


def mixer_kernel(
    xin, w0, w1, w2, w3, w4, w5, wr, wc, dk_in, v0, v1, v2, v3, v4, gain_in, cos_in, sin_in, base_in, df, db, out,
    xin_v, w_v, wr_v, wc_v, xg, nrm, wt, wo, dk, pv, gain, cosine, sine, base, dec, decp, qs, inner, gs, us, st, sp, chip, sg, halo,
    pad, filt, stat, stats, both, part, acc,
    a2m, a2p, am, ap, ta, u, ua, b2m, b2p, bm, bp, bo, tb, v, vb, ss, rs,
):
    pv_in = (v0, v1, v2, v3, v4)
    x, y, z, c = place()
    n = z * 2 + c
    ct, yl = y // 2, y % 2
    xp, xm, x2 = (x + 1) % 4, (x + 3) % 4, (x + 2) % 4
    yp, ym, y2 = (y + 1) % 4, (y + 3) % 4, (y + 2) % 4
    zp, zm = (z + 1) % 8, (z + 7) % 8
    post = Post(ss, rs)
    partner = at(x, y, z, 1 - c)
    loads = list(zip((xin, w0, w1, w2, w3, w4, w5, wr, wc), (xin_v, *(w_v.at[i] for i in range(6)), wr_v, wc_v)))
    for i, (src, dst) in enumerate(loads):
        post.local(("load", i), src, dst)
    own = ct == c
    other = ct != c
    mine = (x * 2 + c) * 512
    s = z * 4 + y
    for p in (0, 1):
        post.key(("w", p, 0)), post.key(("w", p, 1))

    def wsem(p, sub):
        return rs.at[post.ids[("w", p, 0)] + sub]

    group_cols = (pl.ds(0, 512), pl.ds(512, 256))
    for m, w in enumerate((w0, w1, w2, w3, w4, w5)):
        src, dst = w.at[:, cols_at(yl * 128, 128)], wt.at[rows_at(s * 128, 128), pl.ds(m * 128, 128)]
        post.local("w", src, dst, own, wsem(m // 4, yl))
    post.local("gain", gain_in, gain)
    post.local("cos", cos_in, cosine)
    post.local("sin", sin_in, sine)
    post.local("base", base_in, base)
    line = [(dz, (z + dz) % 8) for dz in range(1, 8)]
    greet(
        [at(q, y, z, k) for q in (xp, xm) for k in (0, 1)]
        + [at(x, q, z, k) for q in (yp, ym, y2) for k in (0, 1)]
        + [at(x, y, zp, c), at(x, y, zm, c), partner]
    )

    def xblock(yy, half, r0, rn, col, width):
        return xg.at[rows_at((yy % 2) * 256 + half * SPLIT + r0, rn), cols_at(col, width)]

    for i, (_, dst) in enumerate(loads):
        post.recv(("load", i), dst)

    def wstart(near, p):
        j = 1 - yl if near else yl
        to = at(x, 2 * c + j, z, ct)
        for m in (range(4), range(4, 6))[p]:
            src, dst = w_v.at[m, :, cols_at(j * 128, 128)], wt.at[rows_at(s * 128, 128), pl.ds(m * 128, 128)]
            if near:
                post.send("w", src, dst, to, None, wsem(p, yl))
            else:
                post.send("w", src, dst, to, other, wsem(p, yl))

    def ostart(near):
        j = 1 - yl if near else yl
        to = at(x, 2 * c + j, z, ct)
        for m, (w, w_here) in enumerate(((wr_v, wr), (wc_v, wc))):
            src, dst = w.at[rows_at(j * 128, 128), :], wo.at[pl.ds(m * 128, 128), cols_at(s * 128, 128)]
            if near:
                post.send("o", src, dst, to)
            else:
                post.local("o", w_here.at[rows_at(j * 128, 128), :], dst, own)
                post.send("o", src, dst, to, other)

    wstart(True, 0)
    for half, name, ends in ((1, "x2", ((x, yp, "m"), (x, ym, "p"))), (0, "x1", ((xp, y, "m"), (xm, y, "p")))):
        size = ROWS // 2 - SPLIT if half else SPLIT
        src, dst = xin_v.at[pl.ds(half * SPLIT, size), :], xblock(y, half, 0, size, mine, 512)
        for qx, qy, d in ends:
            post.send(name + d, src, dst, at(qx, qy, z, ct))
        post.send(name + "l", src, dst, partner, other)
        post.local(name + "s", xin.at[pl.ds(half * SPLIT, size), :], dst, own)
    wstart(False, 0)
    wstart(True, 1)
    wstart(False, 1)
    for name, ref, dst in (("dk", dk_in, dk), *((("v", i), r, pv.at[i]) for i, r in enumerate(pv_in))):
        src = ref.at[:, cols_at(yl * 128, 128)]
        post.send(name, src, dst, partner, own)
        post.local(name, src, dst, own)
    decp[0:1, :] = log_sigmoid(jnp.full((1, 128), df[yl], F32))
    decp[1:2, :] = log_sigmoid(jnp.full((1, 128), db[yl], F32))

    first = (yl + c + ct) % 2

    def wrows(zz, i, p, r0=0, rn=128):
        sub = first if i == 0 else 1 - first
        return wt.at[rows_at((zz * 4 + 2 * c + sub) * 128 + r0, rn), group_cols[p]]

    def zsend(zz, i, r, d, p, r0=0, rn=128):
        ref = wrows(zz, i, p, r0, rn)
        post.send(("z", p, d, r, i), ref, ref, at(x, y, zp if d == "m" else zm, c))

    def zpass(zz, i, rel, p, r0=0, rn=128):
        ref = wrows(zz, i, p, r0, rn)
        post.send(("zp", p, rel, i, r0), ref, ref, partner)

    def ocols(zz, i, core=c):
        return wo.at[:, cols_at((zz * 4 + 2 * core + i) * 128, 128)]

    def osend(zz, i, r, d):
        post.send(("o", d, r, i), ocols(zz, i), ocols(zz, i), at(x, y, zp if d == "m" else zm, c))

    def opass(zz, i, rel):
        post.send(("op", rel, i), ocols(zz, i), ocols(zz, i), partner)

    def wfirst(i, p):
        post.recv("w", wrows(z, i, p), None, wsem(p, first if i == 0 else 1 - first))
        for d in ("m", "p"):
            zsend(z, i, 1, d, p)
        zpass(z, i, 0, p)

    def zstep(r, parts, p):
        for i in parts:
            for d in ("m", "p"):
                zz = (z - r) % 8 if d == "m" else (z + r) % 8
                post.recv(("z", p, d, r, i), wrows(zz, i, p))
                if r < 3:
                    zsend(zz, i, r + 1, d, p)
                else:
                    zsend(zz, i, 4, d, p, 0 if d == "m" else 64, 64)
                zpass(zz, i, -r % 8 if d == "m" else r, p)

    far = (z + 4) % 8

    def zfar(i, p):
        for d, r0 in (("m", 0), ("p", 64)):
            post.recv(("z", p, d, 4, i), wrows(far, i, p, r0, 64))
            zpass(far, i, 4, p, r0, 64)

    wfirst(0, 0)
    cm, cp, c2 = ym // 2 == c, yp // 2 == c, y2 // 2 == c
    near, far_ = SPLIT // 2, (ROWS // 2 - SPLIT) // 2

    def x1(qx, r0=0, rn=SPLIT):
        return xblock(y, 0, r0, rn, qx * 1024, 1024)

    def x2b(yy, r0=0, rn=ROWS // 2 - SPLIT):
        return xblock(yy, 1, r0, rn, x * 1024, 1024)

    def x3(yy, qx, r0=0, rn=SPLIT):
        return xblock(yy, 0, r0, rn, qx * 1024, 1024)

    def x4(qx, i, r0=0, rn=ROWS // 2 - SPLIT):
        return xblock(first if i == 0 else 1 - first, 1, r0, rn, qx * 1024, 1024)

    def x3send(i, qx):
        for d, q in (("m", yp), ("p", ym)):
            post.send(("x3" + d, i), x3(y, qx), x3(y, qx), at(x, q, z, c), own)

    def x4send(i, cond):
        for d, q in (("m", xp), ("p", xm)):
            post.send(("x4" + d, i), x4(x, i), x4(x, i), at(q, y, z, c), cond)

    for name, half, size in (("x1", 0, SPLIT), ("x2", 1, ROWS // 2 - SPLIT)):
        post.recv(name + "s", xblock(y, half, 0, size, mine, 512), own)
        post.recv(name + "l", xblock(y, half, 0, size, (x * 2 + 1 - c) * 512, 512), own)
    x4send(0, own)
    post.recv("x1m", x1(xm), own)
    post.send("x1m2", x1(xm, 0, near), x1(xm, 0, near), at(xp, y, z, c), own)
    post.recv("x1p", x1(xp), own)
    post.send("x1p2", x1(xp, near, near), x1(xp, near, near), at(xm, y, z, c), own)
    wfirst(1, 0)
    post.recv("x2m", x2b(ym), cm)
    post.send("x2m2", x2b(ym, 0, far_), x2b(ym, 0, far_), at(x, yp, z, c), cm)
    post.recv("x2p", x2b(yp), cp)
    post.send("x2p2", x2b(yp, far_, far_), x2b(yp, far_, far_), at(x, ym, z, c), cp)
    x4send(0, other)
    x4send(1, own)
    x3send(0, x)
    x3send(1, xm)
    x3send(2, xp)
    zstep(1, (0,), 0)
    post.recv("x1m2", x1(x2, 0, near), own)
    post.recv("x1p2", x1(x2, near, near), own)
    x3send(3, x2)
    zstep(1, (1,), 0)
    post.recv("x2m2", x2b(y2, 0, far_), c2)
    post.recv("x2p2", x2b(y2, far_, far_), c2)
    x4send(1, other)
    ostart(True)
    ostart(False)
    post.send("dec", decp, dec, partner, own)

    def x3pass(i, qx):
        post.recv(("x3m", i), x3(ym, qx), cm)
        ref = x3(ym, qx, 0, near)
        post.send(("x3m2", i), ref, ref, at(x, yp, z, c), cm)
        post.recv(("x3p", i), x3(yp, qx), cp)
        ref = x3(yp, qx, near, near)
        post.send(("x3p2", i), ref, ref, at(x, ym, z, c), cp)

    def x4pass(i):
        post.recv(("x4m", i), x4(xm, i))
        ref = x4(xm, i, 0, far_)
        post.send(("x4m2", i), ref, ref, at(xp, y, z, c))
        post.recv(("x4p", i), x4(xp, i))
        ref = x4(xp, i, far_, far_)
        post.send(("x4p2", i), ref, ref, at(xm, y, z, c))

    def ostep(r, i):
        for d in ("m", "p"):
            zz = (z - r) % 8 if d == "m" else (z + r) % 8
            if r == 4 and i != (d == "p"):
                continue
            post.recv(("o", d, r, i), ocols(zz, i))
            if r < 3 or (r == 3 and i == (d == "p")):
                osend(zz, i, r + 1, d)
            opass(zz, i, -r % 8 if d == "m" else r)

    x4pass(0)
    x3pass(0, x)
    zstep(2, (0,), 0)
    x3pass(1, xm)
    zstep(2, (1,), 0)
    wfirst(0, 1)
    wfirst(1, 1)
    x3pass(2, xp)
    x4pass(1)
    zstep(3, (0,), 0)
    x3pass(3, x2)
    zstep(3, (1,), 0)
    post.recv("o", wo.at[:, cols_at((z * 4 + 2 * c) * 128, 256)])
    for i, qx in enumerate((x, xm, xp, x2)):
        post.recv(("x3m2", i), x3(y2, qx, 0, near), c2)
        post.recv(("x3p2", i), x3(y2, qx, near, near), c2)
    for i in (0, 1):
        post.recv(("x4m2", i), x4(x2, i, 0, far_))
        post.recv(("x4p2", i), x4(x2, i, far_, far_))
    for name, ref in (("gain", gain), ("cos", cosine), ("sin", sine), ("base", base), ("dk", dk), *((("v", i), pv.at[i]) for i in range(5))):
        post.recv(name, ref)

    zstep(1, (0, 1), 1)

    @pl.loop(0, ROWS // 128)
    def _(i):
        rows = rows_at(i * 128, 128)
        square = jnp.zeros((128, 128), F32)
        for k in range(32):
            piece = xg[rows, k * 128 : k * 128 + 128].astype(F32)
            square = square + piece * piece
        scale = lax.rsqrt(jnp.sum(square, axis=1, keepdims=True) / 4096 + EPS)
        for k in range(32):
            cols = slice(k * 128, k * 128 + 128)
            nrm[rows, cols] = (xg[rows, cols].astype(F32) * scale * gain[:, cols]).astype(BF)

    def projects(p, *rels):
        for rel in rels:
            zz = (z + rel) % 8
            for i in (0, 1):
                sub = 1 - first if i == 0 else first
                for r0, rn in ((0, 64), (64, 64)) if rel == 4 else ((0, 128),):
                    row = (zz * 4 + 2 * (1 - c) + sub) * 128 + r0
                    post.recv(("zp", p, rel, i, r0), wt.at[rows_at(row, rn), group_cols[p]])
            cols = slice(512 * p, 512 + 256 * p)
            value = dot(nrm[:, cols_at(zz * 512, 512)], wt[rows_at(zz * 512, 512), cols])
            acc[:, cols] = value if rel == 0 else acc[:, cols] + value

    for i in (0, 1):
        zfar(i, 0)
    projects(0, 0, 1, 7)
    zstep(2, (0, 1), 1)
    projects(0, 2, 6, 3)
    post.recv("dec", dec, other)

    @pl.when(own)
    def _():
        dec[...] = decp[...]

    projects(0, 5, 4)
    proj = acc[:, 0:512].astype(BF)
    cb, sb = base[n][:, 0:128], base[n][:, 128:256]
    cosine[...], sine[...] = cosine[...] * cb - sine[...] * sb, sine[...] * cb + cosine[...] * sb

    def turn(rows):
        wide = rows.astype(F32)
        return (wide * cosine[...] + pltpu.roll(wide, 64, axis=1) * sine[...]).astype(BF)

    keys, values = turn(proj[:, 0:128]), proj[:, 128:256]
    us[...] = (proj[:, 256:384].astype(F32) * jax.nn.sigmoid(proj[:, 384:512].astype(F32))).astype(BF)
    after, before = (n + 1) % 16, (n + 15) % 16
    post.send("ht", us.at[pl.ds(ROWS - 16, 16), :], halo.at[0], at(x, y, after // 2, after % 2))
    post.send("hh", us.at[pl.ds(0, 16), :], halo.at[1], at(x, y, before // 2, before % 2))
    lf, lb = dec[0:1, :], dec[1:2, :]
    place_ = lax.broadcasted_iota(jnp.int32, (ROWS, 128), 0).astype(F32)
    wide = keys.astype(F32)
    st[0] = dot((wide * jnp.exp(lb * place_)).astype(BF), values, ((0,), (0,))).astype(BF)
    st[1] = dot((wide * jnp.exp(lf * (ROWS - 1.0 - place_))).astype(BF), values, ((0,), (0,))).astype(BF)
    post.send("sp", st, sp, partner)
    zstep(3, (0, 1), 1)
    post.recv("sp", sp)
    span = jnp.exp(jnp.where(c == 1, lf, lb) * float(ROWS))
    chip[...] = (st[c].astype(F32) + span * sp[c].astype(F32)).astype(BF)

    def meant(a, b):
        return (a < b) == (c == 1)

    for dz, q in line:
        post.send(("st", dz), chip, sg.at[z], at(x, y, q, c), meant(z, q))
    for i in (0, 1):
        for d in ("m", "p"):
            osend(z, i, 1, d)
    for i in (0, 1):
        opass(z, i, 0)

    post.recv("ht", halo.at[0])
    post.recv("hh", halo.at[1])
    pad[0:16, :] = jnp.where(n > 0, halo[0].astype(F32), 0.0)
    pad[16 : 16 + ROWS, :] = us[...].astype(F32)
    pad[16 + ROWS :, :] = jnp.where(n < 15, halo[1].astype(F32), 0.0)
    lane = lax.broadcasted_iota(jnp.int32, (128, 128), 1)
    for i in range(ROWS // 128):
        filtered = jnp.broadcast_to(pv[0], (128, 128))
        for t in range(KERNEL):
            filtered = filtered + dk[t : t + 1, :] * pad[i * 128 + t + 1 : i * 128 + t + 129, :]
        filt[i * 128 : i * 128 + 128, :] = filtered
        total = jnp.sum(filtered, axis=1, keepdims=True)
        square = jnp.sum(filtered * filtered, axis=1, keepdims=True)
        tile = jnp.where(lane == 0, total, jnp.where(lane == 1, square, 0.0))
        stat[:, i * 128 : i * 128 + 128] = tile.T[0:8, :]
    me = x * 4 + y
    for i in range(4):
        for j in range(4):
            if i or j:
                post.send("stats", stat, stats.at[me], at((x + i) % 4, (y + j) % 4, z, c))
    stats[pl.ds(me, 1)] = stat[...][None]
    projects(1, 0, 1, 7, 2, 6)
    for i in (0, 1):
        zfar(i, 1)
    projects(1, 3, 5)
    projects(1, 4)
    proj = acc[:, 512:768].astype(BF)
    queries = turn(proj[:, 0:128])
    gs[...] = proj[:, 128:256]
    qs[...] = queries
    f1, b1 = lf[:, 0:1], lb[:, 0:1]
    for i in range(ROWS // 128):
        rows = slice(i * 128, i * 128 + 128)
        gap = (
            lax.broadcasted_iota(jnp.int32, (128, ROWS), 0)
            + i * 128
            - lax.broadcasted_iota(jnp.int32, (128, ROWS), 1)
        ).astype(F32)
        decay = jnp.exp(jnp.where(gap >= 0, f1 * gap, -b1 * gap))
        scores = dot(queries[rows], keys, ((1,), (1,))) * decay
        inner[rows, :] = dot(scores.astype(BF), values)
    ostep(1, 0)
    ostep(1, 1)
    for dz, q in line:
        source = (z - dz) % 8
        slot = sg.at[source]
        post.recv(("st", dz), slot, meant(source, z))
        post.send(("ss", dz), slot, slot, partner, meant(source, z))
    sg[pl.ds(z, 1)] = jnp.zeros((1, 128, 128), BF)
    for dz, q in line:
        source = (z - dz) % 8
        post.recv(("ss", dz), sg.at[source], jnp.logical_not(meant(source, z)))
    enter_f, enter_b = jnp.zeros((128, 128), F32), jnp.zeros((128, 128), F32)
    for j in range(8):
        state = sg[j].astype(F32)
        ahead, behind = z - 1 - j, j - z - 1
        wf = jnp.exp(lf * (2 * ROWS * jnp.maximum(ahead, 0)).astype(F32))
        wb_ = jnp.exp(lb * (2 * ROWS * jnp.maximum(behind, 0)).astype(F32))
        enter_f = enter_f + jnp.where(ahead >= 0, wf, 0.0) * state
        enter_b = enter_b + jnp.where(behind >= 0, wb_, 0.0) * state
    enter_f = jnp.where(c == 1, jnp.exp(lf * float(ROWS)) * enter_f + sp[1].astype(F32), enter_f)
    enter_b = jnp.where(c == 0, jnp.exp(lb * float(ROWS)) * enter_b + sp[0].astype(F32), enter_b)
    wide = qs[...].astype(F32)
    retained = inner[...]
    retained = retained + dot((wide * jnp.exp(lf * (place_ + 1.0))).astype(BF), enter_f.astype(BF))
    retained = retained + dot((wide * jnp.exp(lb * (ROWS - place_))).astype(BF), enter_b.astype(BF))
    mean = jnp.mean(retained, axis=-1, keepdims=True)
    centered = retained - mean
    variance = jnp.mean(centered * centered, axis=-1, keepdims=True)
    scaled = centered * lax.rsqrt(variance + EPS) * pv[3] + pv[4]
    both[:, 0:128] = (jax.nn.silu(gs[...].astype(F32)) * scaled).astype(BF)

    post.recv("stats", stats.at[pl.ds(0, 15)])
    total = stats[0]
    for j in range(1, 16):
        total = total + stats[j]
    for i in range(ROWS // 128):
        rows = slice(i * 128, i * 128 + 128)
        tall = jnp.concatenate([total[:, rows], jnp.zeros((120, 128), F32)], axis=0).T
        mean = tall[:, 0:1] / CONV_WIDTH
        variance = tall[:, 1:2] / CONV_WIDTH - mean * mean
        leveled = (filt[rows, :] - mean) * lax.rsqrt(variance + EPS) * pv[1] + pv[2]
        both[rows, 128:256] = jax.nn.silu(leveled).astype(BF)
    def out_part(slots):
        for k in slots:
            zz = (z + ORDER[k]) % 8
            for i in (0, 1):
                post.recv(("op", ORDER[k], i), ocols(zz, i, 1 - c))
            cols = slice(k * 512, k * 512 + 512)
            value = dot(both[...], wo[:, cols_at(zz * 512, 512)])
            part[:, :, :, :, cols] = value.astype(BF).reshape(2, 4, 2, 32, 512)

    to_xp, to_xm = at(xp, y, z, c), at(xm, y, z, c)
    c1p, c1m = cp, cm
    groups = (pl.ds(0, 1536), pl.ds(1536, 1024))

    def add(a, b):
        return (a.astype(F32) + b.astype(F32)).astype(BF)

    def afirst(g):
        cols = groups[g]
        post.send(("a2m", g), part.at[0, x2, :, :, cols], a2m.at[:, :, cols], to_xp)
        post.send(("a2p", g), part.at[1, x2, :, :, cols], a2p.at[:, :, cols], to_xm)
        post.send(("am1", g), part.at[1, xp, :, :, cols], am.at[1, :, :, cols], to_xp)
        post.send(("ap0", g), part.at[0, xm, :, :, cols], ap.at[0, :, :, cols], to_xm)

    def asecond(g):
        cols = groups[g]
        post.recv(("a2m", g), a2m.at[:, :, cols])
        ta[0, :, :, cols] = add(a2m[:, :, cols], part[0, xp, :, :, cols])
        post.send(("am0", g), ta.at[0, :, :, cols], am.at[0, :, :, cols], to_xp)
        post.recv(("a2p", g), a2p.at[:, :, cols])
        ta[1, :, :, cols] = add(a2p[:, :, cols], part[1, xm, :, :, cols])
        post.send(("ap1", g), ta.at[1, :, :, cols], ap.at[1, :, :, cols], to_xm)

    def athird(g):
        cols = groups[g]
        for name, ref in (("am1", am.at[1]), ("ap0", ap.at[0]), ("am0", am.at[0]), ("ap1", ap.at[1])):
            post.recv((name, g), ref.at[:, :, cols])
        for k in (0, 1):
            value = part[k, x, :, :, cols].astype(F32) + am[k, :, :, cols].astype(F32)
            u[k, :, :, cols] = (value + ap[k, :, :, cols].astype(F32)).astype(BF)
        for k in (0, 1):
            for k2 in (0, 1):
                q = 2 * c + k
                here = (q == y) & (k2 == c)
                src, dst = u.at[k, k2, :, cols], ua.at[y, :, cols]
                post.send(("ua", g), src, dst, at(x, q, z, k2), jnp.logical_not(here))
                post.local(("ua", g), src, dst, here)

    def alast(g):
        cols = groups[g]
        post.recv(("ua", g), ua.at[:, :, cols])
        for k in range(cols.start // 512, (cols.start + cols.size) // 512):
            piece = slice(k * 512, k * 512 + 512)
            value = ua[0, :, piece].astype(F32)
            for q in (1, 2, 3):
                value = value + ua[q, :, piece].astype(F32)
            out[:, cols_at(((z + ORDER[k]) % 8) * 512, 512)] = value.astype(BF)

    bgroups = ((0, 1024), (1024, 512))

    def pb(yy, q0, k, g):
        return part.at[yy % 2, pl.ds(q0, 2), k, :, pl.ds(2560 + bgroups[g][0], bgroups[g][1])]

    def bfirst(g):
        cols, size = pl.ds(*bgroups[g]), bgroups[g][1]
        whole = pl.ds(2560 + bgroups[g][0], size)
        for k in (0, 1):
            post.send(("b2m", g), pb(y2, 0, k, g), b2m.at[k, :, :, cols], at(x, yp, z, c), c2)
            post.send(("b2p", g), pb(y2, 2, k, g), b2p.at[k, :, :, cols], at(x, ym, z, c), c2)
        for k in (0, 1):
            post.send(("bm1", g), pb(yp, 2, k, g), bm.at[pl.ds(2, 2), :, cols], at(x, yp, z, k), c1p)
            post.send(("bp0", g), pb(ym, 0, k, g), bp.at[pl.ds(0, 2), :, cols], at(x, ym, z, k), c1m)
        post.send(("bo", g), part.at[y % 2, :, 1 - c, :, whole], bo.at[:, :, cols], partner, own)

        @pl.when(own)
        def _():
            bo[:, :, cols] = part[y % 2, :, c, :, whole]

    def bsecond(g):
        cols = pl.ds(*bgroups[g])
        whole = pl.ds(2560 + bgroups[g][0], bgroups[g][1])
        for name, ref, yy, q0, slot, cond, qy, dst in (
            ("b2m", b2m, yp, 0, 0, c1p, yp, bm),
            ("b2p", b2p, ym, 2, 1, c1m, ym, bp),
        ):
            post.recv((name, g), ref.at[:, :, :, cols], cond)

            @pl.when(cond)
            def _():
                for k in (0, 1):
                    tb[slot, k, :, :, cols] = add(ref[k, :, :, cols], part[yy % 2, q0 : q0 + 2, k, :, whole])

            for k in (0, 1):
                src = tb.at[slot, k, :, :, cols]
                post.send((name, "sum", g), src, dst.at[pl.ds(q0, 2), :, cols], at(x, qy, z, k), cond)

    def bthird(g):
        cols = pl.ds(*bgroups[g])
        post.recv(("bm1", g), bm.at[pl.ds(2, 2), :, cols])
        post.recv(("bp0", g), bp.at[pl.ds(0, 2), :, cols])
        post.recv(("bo", g), bo.at[:, :, cols], other)
        post.recv(("b2m", "sum", g), bm.at[pl.ds(0, 2), :, cols])
        post.recv(("b2p", "sum", g), bp.at[pl.ds(2, 2), :, cols])
        for q in range(4):
            value = bm[q, :, cols].astype(F32) + bp[q, :, cols].astype(F32)
            v[q, :, cols] = (value + bo[q, :, cols].astype(F32)).astype(BF)
        for q in (x2, xp, xm):
            post.send(("vb", g), v.at[q, :, cols], vb.at[x, :, cols], at(q, y, z, c))
        vb[pl.ds(x, 1), :, cols] = v[pl.ds(x, 1), :, cols]

    def blast(g):
        cols = pl.ds(*bgroups[g])
        post.recv(("vb", g), vb.at[pl.ds(0, 3), :, cols])
        for k in range(bgroups[g][0] // 512, sum(bgroups[g]) // 512):
            piece = slice(k * 512, k * 512 + 512)
            value = vb[0, :, piece].astype(F32)
            for q in (1, 2, 3):
                value = value + vb[q, :, piece].astype(F32)
            out[:, cols_at(((z + ORDER[k + 5]) % 8) * 512, 512)] = value.astype(BF)

    out_part((0, 1, 2))
    afirst(0)
    ostep(2, 0)
    ostep(2, 1)
    out_part((3, 4))
    afirst(1)
    for i in (0, 1):
        ostep(3, i)
    out_part((5, 6))
    bfirst(0)
    asecond(0)
    for i in (0, 1):
        ostep(4, i)
    out_part((7,))
    bfirst(1)
    bsecond(0)
    asecond(1)
    bsecond(1)
    bthird(0)
    athird(0)
    bthird(1)
    athird(1)
    blast(0)
    alast(0)
    blast(1)
    alast(1)
    post.finish()


def table():
    half = HEAD_DIM // 2
    inverse = np.tile(THETA ** (-np.arange(half) / half), 2)
    sign = np.repeat([-1.0, 1.0], half)
    near = np.arange(ROWS)[:, None] * inverse
    far = np.arange(16)[:, None] * ROWS * inverse
    base = np.concatenate([np.cos(far), sign * np.sin(far)], axis=1)
    return [a.astype(np.float32) for a in (np.cos(near), sign * np.sin(near), base[:, None])]


def shards(
    hidden_states,
    norm_gain,
    query_weight,
    key_weight,
    value_weight,
    output_gate_weight,
    unit_input_weight,
    unit_gate_weight,
    decay_forward,
    decay_backward,
    group_gain,
    group_bias,
    depth_kernel,
    depth_bias,
    channel_gain,
    channel_bias,
    retention_out_weight,
    convolution_out_weight,
):
    vectors = (depth_bias, channel_gain, channel_bias, group_gain, group_bias)
    wide = lambda *shape: pltpu.VMEM((*shape, 2560), BF)
    narrow = lambda *shape: pltpu.VMEM((*shape, 1536), BF)
    small = lambda dtype: pltpu.VMEM((ROWS, 128), dtype)
    return pl.pallas_call(
        mixer_kernel,
        name="mixer",
        out_shape=jax.ShapeDtypeStruct((32, 4096), BF),
        in_specs=[HBM] * 19 + [SM] * 2,
        out_specs=VM,
        scratch_shapes=[
            pltpu.VMEM((256, 512), BF),
            pltpu.VMEM((6, 128, 256), BF),
            pltpu.VMEM((256, 128), BF),
            pltpu.VMEM((256, 128), BF),
            pltpu.VMEM((ROWS, 4096), BF),
            pltpu.VMEM((ROWS, 4096), BF),
            pltpu.VMEM((4096, 768), BF),
            pltpu.VMEM((256, 4096), BF),
            pltpu.VMEM((KERNEL, 128), F32),
            pltpu.VMEM((5, 1, 128), F32),
            pltpu.VMEM((1, 4096), F32),
            small(F32),
            small(F32),
            pltpu.VMEM((16, 1, 256), F32),
            pltpu.VMEM((8, 128), F32),
            pltpu.VMEM((8, 128), F32),
            small(BF),
            small(F32),
            small(BF),
            small(BF),
            pltpu.VMEM((2, 128, 128), BF),
            pltpu.VMEM((2, 128, 128), BF),
            pltpu.VMEM((128, 128), BF),
            pltpu.VMEM((8, 128, 128), BF),
            pltpu.VMEM((2, 16, 128), BF),
            pltpu.VMEM((ROWS + 32, 128), F32),
            small(F32),
            pltpu.VMEM((8, ROWS), F32),
            pltpu.VMEM((16, 8, ROWS), F32),
            pltpu.VMEM((ROWS, 256), BF),
            pltpu.VMEM((2, 4, 2, 32, 4096), BF),
            pltpu.VMEM((ROWS, 768), F32),
            wide(2, 32),
            wide(2, 32),
            wide(2, 2, 32),
            wide(2, 2, 32),
            wide(2, 2, 32),
            wide(2, 2, 32),
            wide(4, 32),
            narrow(2, 2, 32),
            narrow(2, 2, 32),
            narrow(4, 32),
            narrow(4, 32),
            narrow(4, 32),
            narrow(2, 2, 2, 32),
            narrow(4, 32),
            narrow(4, 32),
            pltpu.SemaphoreType.DMA((340,)),
            pltpu.SemaphoreType.DMA((260,)),
        ],
        compiler_params=pltpu.CompilerParams(
            collective_id=0, has_side_effects=True, vmem_limit_bytes=67043328
        ),
    )(
        hidden_states,
        key_weight,
        value_weight,
        unit_input_weight,
        unit_gate_weight,
        query_weight,
        output_gate_weight,
        retention_out_weight,
        convolution_out_weight,
        depth_kernel,
        *(vector.reshape(1, -1) for vector in vectors),
        norm_gain.reshape(1, -1),
        *table(),
        decay_forward,
        decay_backward,
    )


def solution(mesh):
    split = P("sp", "tp")
    placed = (
        (split, P())
        + (split,) * 6
        + (P("tp"),) * 4
        + (P(None, "tp"),)
        + (P("tp"),) * 3
        + (P("tp", "sp"),) * 2
    )
    return jax.shard_map(
        shards, mesh=mesh, in_specs=placed, out_specs=P(("sp", "tp"), None), check_vma=False
    )
```

```python
import functools

import jax
import jax.numpy as jnp
import numpy as np
from jax import lax
from jax.experimental import pallas as pl
from jax.experimental.pallas import tpu as pltpu
from jax.sharding import PartitionSpec as P

HEAD_DIM = 128
CONV_WIDTH = 2048
KERNEL = 31
EPS = 1e-06
THETA = 10000.0
ROWS = 512
SPLIT = 96
ORDER = (0, 1, 7, 2, 6, 3, 5, 4)
BF = jnp.bfloat16
F32 = jnp.float32
MESH = pl.DeviceIdType.MESH
VM = pl.BlockSpec(memory_space=pltpu.VMEM)
HBM = pl.BlockSpec(memory_space=pltpu.HBM)
SM = pl.BlockSpec(memory_space=pltpu.SMEM)
MIB = 1 << 20


def place():
    sp, tp = lax.axis_index("sp"), lax.axis_index("tp")
    return tp // 2, sp % 4, sp // 4, tp % 2


def at(x, y, z, c):
    return (z * 4 + y, x * 2 + c)


def when(cond, f):
    if cond is None:
        f()
    else:
        pl.when(cond)(f)


class Post:
    def __init__(self, send_sems, recv_sems):
        self.ss, self.rs = send_sems, recv_sems
        self.sent, self.ids = [], {}

    def key(self, name):
        return self.rs.at[self.ids.setdefault(name, len(self.ids))]

    def send(self, name, src, dst, to, cond=None, recv=None):
        sem = self.ss.at[len(self.sent)]
        recv = self.key(name) if recv is None else recv

        def make():
            return pltpu.make_async_remote_copy(
                src_ref=src, dst_ref=dst, send_sem=sem, recv_sem=recv, device_id=to, device_id_type=MESH
            )

        self.sent.append((make, cond))
        when(cond, lambda: make().start())

    def local(self, name, src, dst, cond=None, recv=None):
        recv = self.key(name) if recv is None else recv
        when(cond, lambda: pltpu.make_async_copy(src, dst, recv).start())

    def recv(self, name, ref, cond=None, recv=None):
        recv = self.key(name) if recv is None else recv
        when(cond, lambda: pltpu.make_async_copy(ref, ref, recv).wait())

    def finish(self):
        for make, cond in self.sent:
            when(cond, lambda: make().wait_send())


def greet(peers):
    barrier = pltpu.get_barrier_semaphore()
    for peer in peers:
        pl.semaphore_signal(barrier, inc=1, device_id=peer, device_id_type=MESH)
    pl.semaphore_wait(barrier, len(peers))


def rows_at(start, size, unit=16):
    return pl.ds(pl.multiple_of(start, unit), size)


def cols_at(start, size):
    return pl.ds(pl.multiple_of(start, 128), size)


def dot(a, b, dims=((1,), (0,))):
    return lax.dot_general(a, b, (dims, ((), ())), preferred_element_type=F32)


def log_sigmoid(decay):
    t = jnp.exp(-decay)
    s = t / (2.0 + t)
    square = s * s
    series = jnp.full_like(s, 1.0 / 15)
    for n in (13, 11, 9, 7, 5, 3, 1):
        series = series * square + 1.0 / n
    return -2.0 * s * series


def mixer_kernel(
    xin, w0, w1, w2, w3, w4, w5, wr, wc, dk_in, v0, v1, v2, v3, v4, gain_in, cos_in, sin_in, base_in, df, db, out,
    xin_v, w_v, wr_v, wc_v, xg, nrm, wt, wo, dk, pv, gain, cosine, sine, base, dec, decp, qs, inner, gs, us, st, sp, chip, sg, halo,
    pad, filt, stat, stats, both, part, acc,
    a2m, a2p, am, ap, ta, u, ua, b2m, b2p, bm, bp, bo, tb, v, vb, ss, rs,
):
    pv_in = (v0, v1, v2, v3, v4)
    x, y, z, c = place()
    n = z * 2 + c
    ct, yl = y // 2, y % 2
    xp, xm, x2 = (x + 1) % 4, (x + 3) % 4, (x + 2) % 4
    yp, ym, y2 = (y + 1) % 4, (y + 3) % 4, (y + 2) % 4
    zp, zm = (z + 1) % 8, (z + 7) % 8
    post = Post(ss, rs)
    partner = at(x, y, z, 1 - c)
    loads = list(zip((xin, w0, w1, w2, w3, w4, w5, wr, wc), (xin_v, *(w_v.at[i] for i in range(6)), wr_v, wc_v)))
    for i, (src, dst) in enumerate(loads):
        post.local(("load", i), src, dst)
    own = ct == c
    other = ct != c
    mine = (x * 2 + c) * 512
    s = z * 4 + y
    for p in (0, 1):
        post.key(("w", p, 0)), post.key(("w", p, 1))

    def wsem(p, sub):
        return rs.at[post.ids[("w", p, 0)] + sub]

    group_cols = (pl.ds(0, 512), pl.ds(512, 256))
    for m, w in enumerate((w0, w1, w2, w3, w4, w5)):
        src, dst = w.at[:, cols_at(yl * 128, 128)], wt.at[rows_at(s * 128, 128), pl.ds(m * 128, 128)]
        post.local("w", src, dst, own, wsem(m // 4, yl))
    post.local("gain", gain_in, gain)
    post.local("cos", cos_in, cosine)
    post.local("sin", sin_in, sine)
    post.local("base", base_in, base)
    line = [(dz, (z + dz) % 8) for dz in range(1, 8)]
    greet(
        [at(q, y, z, k) for q in (xp, xm) for k in (0, 1)]
        + [at(x, q, z, k) for q in (yp, ym, y2) for k in (0, 1)]
        + [at(x, y, zp, c), at(x, y, zm, c), partner]
    )

    def xblock(yy, half, r0, rn, col, width):
        return xg.at[rows_at((yy % 2) * 256 + half * SPLIT + r0, rn), cols_at(col, width)]

    for i, (_, dst) in enumerate(loads):
        post.recv(("load", i), dst)

    def wstart(near, p):
        j = 1 - yl if near else yl
        to = at(x, 2 * c + j, z, ct)
        for m in (range(4), range(4, 6))[p]:
            src, dst = w_v.at[m, :, cols_at(j * 128, 128)], wt.at[rows_at(s * 128, 128), pl.ds(m * 128, 128)]
            if near:
                post.send("w", src, dst, to, None, wsem(p, yl))
            else:
                post.send("w", src, dst, to, other, wsem(p, yl))

    def ostart(near):
        j = 1 - yl if near else yl
        to = at(x, 2 * c + j, z, ct)
        for m, (w, w_here) in enumerate(((wr_v, wr), (wc_v, wc))):
            src, dst = w.at[rows_at(j * 128, 128), :], wo.at[pl.ds(m * 128, 128), cols_at(s * 128, 128)]
            if near:
                post.send("o", src, dst, to)
            else:
                post.local("o", w_here.at[rows_at(j * 128, 128), :], dst, own)
                post.send("o", src, dst, to, other)

    wstart(True, 0)
    for half, name, ends in ((1, "x2", ((x, yp, "m"), (x, ym, "p"))), (0, "x1", ((xp, y, "m"), (xm, y, "p")))):
        size = ROWS // 2 - SPLIT if half else SPLIT
        src, dst = xin_v.at[pl.ds(half * SPLIT, size), :], xblock(y, half, 0, size, mine, 512)
        for qx, qy, d in ends:
            post.send(name + d, src, dst, at(qx, qy, z, ct))
        post.send(name + "l", src, dst, partner, other)
        post.local(name + "s", xin.at[pl.ds(half * SPLIT, size), :], dst, own)
    wstart(False, 0)
    wstart(True, 1)
    wstart(False, 1)
    for name, ref, dst in (("dk", dk_in, dk), *((("v", i), r, pv.at[i]) for i, r in enumerate(pv_in))):
        src = ref.at[:, cols_at(yl * 128, 128)]
        post.send(name, src, dst, partner, own)
        post.local(name, src, dst, own)
    decp[0:1, :] = log_sigmoid(jnp.full((1, 128), df[yl], F32))
    decp[1:2, :] = log_sigmoid(jnp.full((1, 128), db[yl], F32))

    first = (yl + c + ct) % 2

    def wrows(zz, i, p, r0=0, rn=128):
        sub = first if i == 0 else 1 - first
        return wt.at[rows_at((zz * 4 + 2 * c + sub) * 128 + r0, rn), group_cols[p]]

    def zsend(zz, i, r, d, p, r0=0, rn=128):
        ref = wrows(zz, i, p, r0, rn)
        post.send(("z", p, d, r, i), ref, ref, at(x, y, zp if d == "m" else zm, c))

    def zpass(zz, i, rel, p, r0=0, rn=128):
        ref = wrows(zz, i, p, r0, rn)
        post.send(("zp", p, rel, i, r0), ref, ref, partner)

    def ocols(zz, i, core=c):
        return wo.at[:, cols_at((zz * 4 + 2 * core + i) * 128, 128)]

    def osend(zz, i, r, d):
        post.send(("o", d, r, i), ocols(zz, i), ocols(zz, i), at(x, y, zp if d == "m" else zm, c))

    def opass(zz, i, rel):
        post.send(("op", rel, i), ocols(zz, i), ocols(zz, i), partner)

    def wfirst(i, p):
        post.recv("w", wrows(z, i, p), None, wsem(p, first if i == 0 else 1 - first))
        for d in ("m", "p"):
            zsend(z, i, 1, d, p)
        zpass(z, i, 0, p)

    def zstep(r, parts, p):
        for i in parts:
            for d in ("m", "p"):
                zz = (z - r) % 8 if d == "m" else (z + r) % 8
                post.recv(("z", p, d, r, i), wrows(zz, i, p))
                if r < 3:
                    zsend(zz, i, r + 1, d, p)
                else:
                    zsend(zz, i, 4, d, p, 0 if d == "m" else 64, 64)
                zpass(zz, i, -r % 8 if d == "m" else r, p)

    far = (z + 4) % 8

    def zfar(i, p):
        for d, r0 in (("m", 0), ("p", 64)):
            post.recv(("z", p, d, 4, i), wrows(far, i, p, r0, 64))
            zpass(far, i, 4, p, r0, 64)

    wfirst(0, 0)
    cm, cp, c2 = ym // 2 == c, yp // 2 == c, y2 // 2 == c
    near, far_ = SPLIT // 2, (ROWS // 2 - SPLIT) // 2

    def x1(qx, r0=0, rn=SPLIT):
        return xblock(y, 0, r0, rn, qx * 1024, 1024)

    def x2b(yy, r0=0, rn=ROWS // 2 - SPLIT):
        return xblock(yy, 1, r0, rn, x * 1024, 1024)

    def x3(yy, qx, r0=0, rn=SPLIT):
        return xblock(yy, 0, r0, rn, qx * 1024, 1024)

    def x4(qx, i, r0=0, rn=ROWS // 2 - SPLIT):
        return xblock(first if i == 0 else 1 - first, 1, r0, rn, qx * 1024, 1024)

    def x3send(i, qx):
        for d, q in (("m", yp), ("p", ym)):
            post.send(("x3" + d, i), x3(y, qx), x3(y, qx), at(x, q, z, c), own)

    def x4send(i, cond):
        for d, q in (("m", xp), ("p", xm)):
            post.send(("x4" + d, i), x4(x, i), x4(x, i), at(q, y, z, c), cond)

    for name, half, size in (("x1", 0, SPLIT), ("x2", 1, ROWS // 2 - SPLIT)):
        post.recv(name + "s", xblock(y, half, 0, size, mine, 512), own)
        post.recv(name + "l", xblock(y, half, 0, size, (x * 2 + 1 - c) * 512, 512), own)
    x4send(0, own)
    post.recv("x1m", x1(xm), own)
    post.send("x1m2", x1(xm, 0, near), x1(xm, 0, near), at(xp, y, z, c), own)
    post.recv("x1p", x1(xp), own)
    post.send("x1p2", x1(xp, near, near), x1(xp, near, near), at(xm, y, z, c), own)
    wfirst(1, 0)
    post.recv("x2m", x2b(ym), cm)
    post.send("x2m2", x2b(ym, 0, far_), x2b(ym, 0, far_), at(x, yp, z, c), cm)
    post.recv("x2p", x2b(yp), cp)
    post.send("x2p2", x2b(yp, far_, far_), x2b(yp, far_, far_), at(x, ym, z, c), cp)
    x4send(0, other)
    x4send(1, own)
    x3send(0, x)
    x3send(1, xm)
    x3send(2, xp)
    zstep(1, (0,), 0)
    post.recv("x1m2", x1(x2, 0, near), own)
    post.recv("x1p2", x1(x2, near, near), own)
    x3send(3, x2)
    zstep(1, (1,), 0)
    post.recv("x2m2", x2b(y2, 0, far_), c2)
    post.recv("x2p2", x2b(y2, far_, far_), c2)
    x4send(1, other)
    ostart(True)
    ostart(False)
    post.send("dec", decp, dec, partner, own)

    def x3pass(i, qx):
        post.recv(("x3m", i), x3(ym, qx), cm)
        ref = x3(ym, qx, 0, near)
        post.send(("x3m2", i), ref, ref, at(x, yp, z, c), cm)
        post.recv(("x3p", i), x3(yp, qx), cp)
        ref = x3(yp, qx, near, near)
        post.send(("x3p2", i), ref, ref, at(x, ym, z, c), cp)

    def x4pass(i):
        post.recv(("x4m", i), x4(xm, i))
        ref = x4(xm, i, 0, far_)
        post.send(("x4m2", i), ref, ref, at(xp, y, z, c))
        post.recv(("x4p", i), x4(xp, i))
        ref = x4(xp, i, far_, far_)
        post.send(("x4p2", i), ref, ref, at(xm, y, z, c))

    def ostep(r, i):
        for d in ("m", "p"):
            zz = (z - r) % 8 if d == "m" else (z + r) % 8
            if r == 4 and i != (d == "p"):
                continue
            post.recv(("o", d, r, i), ocols(zz, i))
            if r < 3 or (r == 3 and i == (d == "p")):
                osend(zz, i, r + 1, d)
            opass(zz, i, -r % 8 if d == "m" else r)

    zstep(2, (0,), 0)
    x4pass(0)
    x3pass(0, x)
    x3pass(1, xm)
    zstep(2, (1,), 0)
    wfirst(0, 1)
    wfirst(1, 1)
    x3pass(2, xp)
    x4pass(1)
    zstep(3, (0,), 0)
    x3pass(3, x2)
    zstep(3, (1,), 0)
    post.recv("o", wo.at[:, cols_at((z * 4 + 2 * c) * 128, 256)])
    for i, qx in enumerate((x, xm, xp, x2)):
        post.recv(("x3m2", i), x3(y2, qx, 0, near), c2)
        post.recv(("x3p2", i), x3(y2, qx, near, near), c2)
    for i in (0, 1):
        post.recv(("x4m2", i), x4(x2, i, 0, far_))
        post.recv(("x4p2", i), x4(x2, i, far_, far_))
    for name, ref in (("gain", gain), ("cos", cosine), ("sin", sine), ("base", base), ("dk", dk), *((("v", i), pv.at[i]) for i in range(5))):
        post.recv(name, ref)

    zstep(1, (0, 1), 1)

    @pl.loop(0, ROWS // 128)
    def _(i):
        rows = rows_at(i * 128, 128)
        square = jnp.zeros((128, 128), F32)
        for k in range(32):
            piece = xg[rows, k * 128 : k * 128 + 128].astype(F32)
            square = square + piece * piece
        scale = lax.rsqrt(jnp.sum(square, axis=1, keepdims=True) / 4096 + EPS)
        for k in range(32):
            cols = slice(k * 128, k * 128 + 128)
            nrm[rows, cols] = (xg[rows, cols].astype(F32) * scale * gain[:, cols]).astype(BF)

    def projects(p, *rels):
        for rel in rels:
            zz = (z + rel) % 8
            for i in (0, 1):
                sub = 1 - first if i == 0 else first
                for r0, rn in ((0, 64), (64, 64)) if rel == 4 else ((0, 128),):
                    row = (zz * 4 + 2 * (1 - c) + sub) * 128 + r0
                    post.recv(("zp", p, rel, i, r0), wt.at[rows_at(row, rn), group_cols[p]])
            cols = slice(512 * p, 512 + 256 * p)
            value = dot(nrm[:, cols_at(zz * 512, 512)], wt[rows_at(zz * 512, 512), cols])
            acc[:, cols] = value if rel == 0 else acc[:, cols] + value

    for i in (0, 1):
        zfar(i, 0)
    projects(0, 0, 1, 7)
    zstep(2, (0, 1), 1)
    projects(0, 2, 6, 3)
    post.recv("dec", dec, other)

    @pl.when(own)
    def _():
        dec[...] = decp[...]

    projects(0, 5, 4)
    proj = acc[:, 0:512].astype(BF)
    cb, sb = base[n][:, 0:128], base[n][:, 128:256]
    cosine[...], sine[...] = cosine[...] * cb - sine[...] * sb, sine[...] * cb + cosine[...] * sb

    def turn(rows):
        wide = rows.astype(F32)
        return (wide * cosine[...] + pltpu.roll(wide, 64, axis=1) * sine[...]).astype(BF)

    keys, values = turn(proj[:, 0:128]), proj[:, 128:256]
    us[...] = (proj[:, 256:384].astype(F32) * jax.nn.sigmoid(proj[:, 384:512].astype(F32))).astype(BF)
    after, before = (n + 1) % 16, (n + 15) % 16
    post.send("ht", us.at[pl.ds(ROWS - 16, 16), :], halo.at[0], at(x, y, after // 2, after % 2))
    post.send("hh", us.at[pl.ds(0, 16), :], halo.at[1], at(x, y, before // 2, before % 2))
    lf, lb = dec[0:1, :], dec[1:2, :]
    place_ = lax.broadcasted_iota(jnp.int32, (ROWS, 128), 0).astype(F32)
    wide = keys.astype(F32)
    st[0] = dot((wide * jnp.exp(lb * place_)).astype(BF), values, ((0,), (0,))).astype(BF)
    st[1] = dot((wide * jnp.exp(lf * (ROWS - 1.0 - place_))).astype(BF), values, ((0,), (0,))).astype(BF)
    post.send("sp", st, sp, partner)
    zstep(3, (0, 1), 1)
    post.recv("sp", sp)
    span = jnp.exp(jnp.where(c == 1, lf, lb) * float(ROWS))
    chip[...] = (st[c].astype(F32) + span * sp[c].astype(F32)).astype(BF)

    def meant(a, b):
        return (a < b) == (c == 1)

    for dz, q in line:
        post.send(("st", dz), chip, sg.at[z], at(x, y, q, c), meant(z, q))
    for i in (0, 1):
        for d in ("m", "p"):
            osend(z, i, 1, d)
    for i in (0, 1):
        opass(z, i, 0)

    post.recv("ht", halo.at[0])
    post.recv("hh", halo.at[1])
    pad[0:16, :] = jnp.where(n > 0, halo[0].astype(F32), 0.0)
    pad[16 : 16 + ROWS, :] = us[...].astype(F32)
    pad[16 + ROWS :, :] = jnp.where(n < 15, halo[1].astype(F32), 0.0)
    lane = lax.broadcasted_iota(jnp.int32, (128, 128), 1)
    for i in range(ROWS // 128):
        filtered = jnp.broadcast_to(pv[0], (128, 128))
        for t in range(KERNEL):
            filtered = filtered + dk[t : t + 1, :] * pad[i * 128 + t + 1 : i * 128 + t + 129, :]
        filt[i * 128 : i * 128 + 128, :] = filtered
        total = jnp.sum(filtered, axis=1, keepdims=True)
        square = jnp.sum(filtered * filtered, axis=1, keepdims=True)
        tile = jnp.where(lane == 0, total, jnp.where(lane == 1, square, 0.0))
        stat[:, i * 128 : i * 128 + 128] = tile.T[0:8, :]
    me = x * 4 + y
    for i in range(4):
        for j in range(4):
            if i or j:
                post.send("stats", stat, stats.at[me], at((x + i) % 4, (y + j) % 4, z, c))
    stats[pl.ds(me, 1)] = stat[...][None]
    projects(1, 0, 1, 7, 2, 6)
    for i in (0, 1):
        zfar(i, 1)
    projects(1, 3, 5)
    projects(1, 4)
    proj = acc[:, 512:768].astype(BF)
    queries = turn(proj[:, 0:128])
    gs[...] = proj[:, 128:256]
    qs[...] = queries
    f1, b1 = lf[:, 0:1], lb[:, 0:1]
    for i in range(ROWS // 128):
        rows = slice(i * 128, i * 128 + 128)
        gap = (
            lax.broadcasted_iota(jnp.int32, (128, ROWS), 0)
            + i * 128
            - lax.broadcasted_iota(jnp.int32, (128, ROWS), 1)
        ).astype(F32)
        decay = jnp.exp(jnp.where(gap >= 0, f1 * gap, -b1 * gap))
        scores = dot(queries[rows], keys, ((1,), (1,))) * decay
        inner[rows, :] = dot(scores.astype(BF), values)
    ostep(1, 0)
    ostep(1, 1)
    for dz, q in line:
        source = (z - dz) % 8
        slot = sg.at[source]
        post.recv(("st", dz), slot, meant(source, z))
        post.send(("ss", dz), slot, slot, partner, meant(source, z))
    sg[pl.ds(z, 1)] = jnp.zeros((1, 128, 128), BF)
    for dz, q in line:
        source = (z - dz) % 8
        post.recv(("ss", dz), sg.at[source], jnp.logical_not(meant(source, z)))
    enter_f, enter_b = jnp.zeros((128, 128), F32), jnp.zeros((128, 128), F32)
    for j in range(8):
        state = sg[j].astype(F32)
        ahead, behind = z - 1 - j, j - z - 1
        wf = jnp.exp(lf * (2 * ROWS * jnp.maximum(ahead, 0)).astype(F32))
        wb_ = jnp.exp(lb * (2 * ROWS * jnp.maximum(behind, 0)).astype(F32))
        enter_f = enter_f + jnp.where(ahead >= 0, wf, 0.0) * state
        enter_b = enter_b + jnp.where(behind >= 0, wb_, 0.0) * state
    enter_f = jnp.where(c == 1, jnp.exp(lf * float(ROWS)) * enter_f + sp[1].astype(F32), enter_f)
    enter_b = jnp.where(c == 0, jnp.exp(lb * float(ROWS)) * enter_b + sp[0].astype(F32), enter_b)
    wide = qs[...].astype(F32)
    retained = inner[...]
    retained = retained + dot((wide * jnp.exp(lf * (place_ + 1.0))).astype(BF), enter_f.astype(BF))
    retained = retained + dot((wide * jnp.exp(lb * (ROWS - place_))).astype(BF), enter_b.astype(BF))
    mean = jnp.mean(retained, axis=-1, keepdims=True)
    centered = retained - mean
    variance = jnp.mean(centered * centered, axis=-1, keepdims=True)
    scaled = centered * lax.rsqrt(variance + EPS) * pv[3] + pv[4]
    both[:, 0:128] = (jax.nn.silu(gs[...].astype(F32)) * scaled).astype(BF)

    post.recv("stats", stats.at[pl.ds(0, 15)])
    total = stats[0]
    for j in range(1, 16):
        total = total + stats[j]
    for i in range(ROWS // 128):
        rows = slice(i * 128, i * 128 + 128)
        tall = jnp.concatenate([total[:, rows], jnp.zeros((120, 128), F32)], axis=0).T
        mean = tall[:, 0:1] / CONV_WIDTH
        variance = tall[:, 1:2] / CONV_WIDTH - mean * mean
        leveled = (filt[rows, :] - mean) * lax.rsqrt(variance + EPS) * pv[1] + pv[2]
        both[rows, 128:256] = jax.nn.silu(leveled).astype(BF)
    def out_part(slots):
        for k in slots:
            zz = (z + ORDER[k]) % 8
            for i in (0, 1):
                post.recv(("op", ORDER[k], i), ocols(zz, i, 1 - c))
            cols = slice(k * 512, k * 512 + 512)
            value = dot(both[...], wo[:, cols_at(zz * 512, 512)])
            part[:, :, :, :, cols] = value.astype(BF).reshape(2, 4, 2, 32, 512)

    to_xp, to_xm = at(xp, y, z, c), at(xm, y, z, c)
    c1p, c1m = cp, cm
    groups = (pl.ds(0, 1536), pl.ds(1536, 512))

    def add(a, b):
        return (a.astype(F32) + b.astype(F32)).astype(BF)

    def afirst(g):
        cols = groups[g]
        post.send(("a2m", g), part.at[0, x2, :, :, cols], a2m.at[:, :, cols], to_xp)
        post.send(("a2p", g), part.at[1, x2, :, :, cols], a2p.at[:, :, cols], to_xm)
        post.send(("am1", g), part.at[1, xp, :, :, cols], am.at[1, :, :, cols], to_xp)
        post.send(("ap0", g), part.at[0, xm, :, :, cols], ap.at[0, :, :, cols], to_xm)

    def asecond(g):
        cols = groups[g]
        post.recv(("a2m", g), a2m.at[:, :, cols])
        ta[0, :, :, cols] = add(a2m[:, :, cols], part[0, xp, :, :, cols])
        post.send(("am0", g), ta.at[0, :, :, cols], am.at[0, :, :, cols], to_xp)
        post.recv(("a2p", g), a2p.at[:, :, cols])
        ta[1, :, :, cols] = add(a2p[:, :, cols], part[1, xm, :, :, cols])
        post.send(("ap1", g), ta.at[1, :, :, cols], ap.at[1, :, :, cols], to_xm)

    def athird(g):
        cols = groups[g]
        for name, ref in (("am1", am.at[1]), ("ap0", ap.at[0]), ("am0", am.at[0]), ("ap1", ap.at[1])):
            post.recv((name, g), ref.at[:, :, cols])
        for k in (0, 1):
            value = part[k, x, :, :, cols].astype(F32) + am[k, :, :, cols].astype(F32)
            u[k, :, :, cols] = (value + ap[k, :, :, cols].astype(F32)).astype(BF)
        for k in (0, 1):
            for k2 in (0, 1):
                q = 2 * c + k
                here = (q == y) & (k2 == c)
                src, dst = u.at[k, k2, :, cols], ua.at[y, :, cols]
                post.send(("ua", g), src, dst, at(x, q, z, k2), jnp.logical_not(here))
                post.local(("ua", g), src, dst, here)

    def alast(g):
        cols = groups[g]
        post.recv(("ua", g), ua.at[:, :, cols])
        for k in range(cols.start // 512, (cols.start + cols.size) // 512):
            piece = slice(k * 512, k * 512 + 512)
            value = ua[0, :, piece].astype(F32)
            for q in (1, 2, 3):
                value = value + ua[q, :, piece].astype(F32)
            out[:, cols_at(((z + ORDER[k]) % 8) * 512, 512)] = value.astype(BF)

    bgroups = ((0, 512), (512, 1024), (1536, 512))

    def pb(yy, q0, k, g):
        return part.at[yy % 2, pl.ds(q0, 2), k, :, pl.ds(2048 + bgroups[g][0], bgroups[g][1])]

    def bfirst(g):
        cols, size = pl.ds(*bgroups[g]), bgroups[g][1]
        whole = pl.ds(2048 + bgroups[g][0], size)
        for k in (0, 1):
            post.send(("b2m", g), pb(y2, 0, k, g), b2m.at[k, :, :, cols], at(x, yp, z, c), c2)
            post.send(("b2p", g), pb(y2, 2, k, g), b2p.at[k, :, :, cols], at(x, ym, z, c), c2)
        for k in (0, 1):
            post.send(("bm1", g), pb(yp, 2, k, g), bm.at[pl.ds(2, 2), :, cols], at(x, yp, z, k), c1p)
            post.send(("bp0", g), pb(ym, 0, k, g), bp.at[pl.ds(0, 2), :, cols], at(x, ym, z, k), c1m)
        post.send(("bo", g), part.at[y % 2, :, 1 - c, :, whole], bo.at[:, :, cols], partner, own)

        @pl.when(own)
        def _():
            bo[:, :, cols] = part[y % 2, :, c, :, whole]

    def bsecond(g):
        cols = pl.ds(*bgroups[g])
        whole = pl.ds(2048 + bgroups[g][0], bgroups[g][1])
        for name, ref, yy, q0, slot, cond, qy, dst in (
            ("b2m", b2m, yp, 0, 0, c1p, yp, bm),
            ("b2p", b2p, ym, 2, 1, c1m, ym, bp),
        ):
            post.recv((name, g), ref.at[:, :, :, cols], cond)

            @pl.when(cond)
            def _():
                for k in (0, 1):
                    tb[slot, k, :, :, cols] = add(ref[k, :, :, cols], part[yy % 2, q0 : q0 + 2, k, :, whole])

            for k in (0, 1):
                src = tb.at[slot, k, :, :, cols]
                post.send((name, "sum", g), src, dst.at[pl.ds(q0, 2), :, cols], at(x, qy, z, k), cond)

    def bthird(g):
        cols = pl.ds(*bgroups[g])
        post.recv(("bm1", g), bm.at[pl.ds(2, 2), :, cols])
        post.recv(("bp0", g), bp.at[pl.ds(0, 2), :, cols])
        post.recv(("bo", g), bo.at[:, :, cols], other)
        post.recv(("b2m", "sum", g), bm.at[pl.ds(0, 2), :, cols])
        post.recv(("b2p", "sum", g), bp.at[pl.ds(2, 2), :, cols])
        for q in range(4):
            value = bm[q, :, cols].astype(F32) + bp[q, :, cols].astype(F32)
            v[q, :, cols] = (value + bo[q, :, cols].astype(F32)).astype(BF)
        for q in (x2, xp, xm):
            post.send(("vb", g), v.at[q, :, cols], vb.at[x, :, cols], at(q, y, z, c))
        vb[pl.ds(x, 1), :, cols] = v[pl.ds(x, 1), :, cols]

    def blast(g):
        cols = pl.ds(*bgroups[g])
        post.recv(("vb", g), vb.at[pl.ds(0, 3), :, cols])
        for k in range(bgroups[g][0] // 512, sum(bgroups[g]) // 512):
            piece = slice(k * 512, k * 512 + 512)
            value = vb[0, :, piece].astype(F32)
            for q in (1, 2, 3):
                value = value + vb[q, :, piece].astype(F32)
            out[:, cols_at(((z + ORDER[k + 4]) % 8) * 512, 512)] = value.astype(BF)

    out_part((0, 1, 2))
    afirst(0)
    ostep(2, 0)
    ostep(2, 1)
    out_part((3, 4))
    afirst(1)
    bfirst(0)
    for i in (0, 1):
        ostep(3, i)
    out_part((5, 6))
    bfirst(1)
    bsecond(0)
    asecond(0)
    for i in (0, 1):
        ostep(4, i)
    out_part((7,))
    bfirst(2)
    bsecond(1)
    asecond(1)
    bsecond(2)
    bthird(0)
    athird(0)
    bthird(1)
    athird(1)
    bthird(2)
    blast(0)
    alast(0)
    blast(1)
    alast(1)
    blast(2)
    post.finish()


def table():
    half = HEAD_DIM // 2
    inverse = np.tile(THETA ** (-np.arange(half) / half), 2)
    sign = np.repeat([-1.0, 1.0], half)
    near = np.arange(ROWS)[:, None] * inverse
    far = np.arange(16)[:, None] * ROWS * inverse
    base = np.concatenate([np.cos(far), sign * np.sin(far)], axis=1)
    return [a.astype(np.float32) for a in (np.cos(near), sign * np.sin(near), base[:, None])]


def shards(
    hidden_states,
    norm_gain,
    query_weight,
    key_weight,
    value_weight,
    output_gate_weight,
    unit_input_weight,
    unit_gate_weight,
    decay_forward,
    decay_backward,
    group_gain,
    group_bias,
    depth_kernel,
    depth_bias,
    channel_gain,
    channel_bias,
    retention_out_weight,
    convolution_out_weight,
):
    vectors = (depth_bias, channel_gain, channel_bias, group_gain, group_bias)
    wide = lambda *shape: pltpu.VMEM((*shape, 2048), BF)
    narrow = lambda *shape: pltpu.VMEM((*shape, 2048), BF)
    small = lambda dtype: pltpu.VMEM((ROWS, 128), dtype)
    return pl.pallas_call(
        mixer_kernel,
        name="mixer",
        out_shape=jax.ShapeDtypeStruct((32, 4096), BF),
        in_specs=[HBM] * 19 + [SM] * 2,
        out_specs=VM,
        scratch_shapes=[
            pltpu.VMEM((256, 512), BF),
            pltpu.VMEM((6, 128, 256), BF),
            pltpu.VMEM((256, 128), BF),
            pltpu.VMEM((256, 128), BF),
            pltpu.VMEM((ROWS, 4096), BF),
            pltpu.VMEM((ROWS, 4096), BF),
            pltpu.VMEM((4096, 768), BF),
            pltpu.VMEM((256, 4096), BF),
            pltpu.VMEM((KERNEL, 128), F32),
            pltpu.VMEM((5, 1, 128), F32),
            pltpu.VMEM((1, 4096), F32),
            small(F32),
            small(F32),
            pltpu.VMEM((16, 1, 256), F32),
            pltpu.VMEM((8, 128), F32),
            pltpu.VMEM((8, 128), F32),
            small(BF),
            small(F32),
            small(BF),
            small(BF),
            pltpu.VMEM((2, 128, 128), BF),
            pltpu.VMEM((2, 128, 128), BF),
            pltpu.VMEM((128, 128), BF),
            pltpu.VMEM((8, 128, 128), BF),
            pltpu.VMEM((2, 16, 128), BF),
            pltpu.VMEM((ROWS + 32, 128), F32),
            small(F32),
            pltpu.VMEM((8, ROWS), F32),
            pltpu.VMEM((16, 8, ROWS), F32),
            pltpu.VMEM((ROWS, 256), BF),
            pltpu.VMEM((2, 4, 2, 32, 4096), BF),
            pltpu.VMEM((ROWS, 768), F32),
            wide(2, 32),
            wide(2, 32),
            wide(2, 2, 32),
            wide(2, 2, 32),
            wide(2, 2, 32),
            wide(2, 2, 32),
            wide(4, 32),
            narrow(2, 2, 32),
            narrow(2, 2, 32),
            narrow(4, 32),
            narrow(4, 32),
            narrow(4, 32),
            narrow(2, 2, 2, 32),
            narrow(4, 32),
            narrow(4, 32),
            pltpu.SemaphoreType.DMA((360,)),
            pltpu.SemaphoreType.DMA((280,)),
        ],
        compiler_params=pltpu.CompilerParams(
            collective_id=0, has_side_effects=True, vmem_limit_bytes=67043328
        ),
    )(
        hidden_states,
        key_weight,
        value_weight,
        unit_input_weight,
        unit_gate_weight,
        query_weight,
        output_gate_weight,
        retention_out_weight,
        convolution_out_weight,
        depth_kernel,
        *(vector.reshape(1, -1) for vector in vectors),
        norm_gain.reshape(1, -1),
        *table(),
        decay_forward,
        decay_backward,
    )


def solution(mesh):
    split = P("sp", "tp")
    placed = (
        (split, P())
        + (split,) * 6
        + (P("tp"),) * 4
        + (P(None, "tp"),)
        + (P("tp"),) * 3
        + (P("tp", "sp"),) * 2
    )
    return jax.shard_map(
        shards, mesh=mesh, in_specs=placed, out_specs=P(("sp", "tp"), None), check_vma=False
    )
```
